256 devices in a mesh: sp: 32 (over z, x), tp: 8 (over y, core).
Axes of the slice: x: 4, y: 4, z: 8, core: 2. Of those that a mesh axis runs over, the one named last changes fastest.
Arguments:
- tokens: bfloat16 [2, 6144, 4096], P(None, 'sp', 'tp'), may hold values from -12 to 12
- query_weight: bfloat16 [4096, 2048], P(None, 'tp'), may hold values from -0.09375 to 0.09375
- key_weight: bfloat16 [4096, 2048], P(None, 'tp'), may hold values from -0.09375 to 0.09375
- value_weight: bfloat16 [4096, 2048], P(None, 'tp'), may hold values from -0.09375 to 0.09375
- gate_weight: bfloat16 [4096, 2048], P(None, 'tp'), may hold values from -0.09375 to 0.09375
- beta_weight: bfloat16 [4096, 16], P(None, 'tp'), may hold values from -0.09375 to 0.09375
- decay_weight: bfloat16 [4096, 16], P(None, 'tp'), may hold values from -0.09375 to 0.09375
- beta_bias: float32 [16], P('tp'), may hold values from -6 to -3
- rate_log: float32 [16], P('tp'), may hold values from -12 to -2.5
- out_gain: float32 [128], replicated, may hold values from 0.1 to 1.9
- new_query: bfloat16 [2, 16, 128], P(None, 'tp'), may hold values from -6 to 6
- new_key: bfloat16 [2, 16, 128], P(None, 'tp'), may hold values from -6 to 6
- new_value: bfloat16 [2, 16, 128], P(None, 'tp'), may hold values from -6 to 6
- new_beta: float32 [2, 16], P(None, 'tp'), may hold values from 0.1 to 0.9
- new_decay: float32 [2, 16], P(None, 'tp'), may hold values from 0.3 to 1
Outputs:
- mixed_out: bfloat16 [2, 6144, 2048], P(None, 'sp', 'tp')
- cache: bfloat16 [2, 16, 128, 128], P(None, 'tp', 'sp')
- first_out: float32 [2, 2048], P(None, 'tp')
The draws below stay inside these ranges and needn't reach their ends.
All inputs are finite; a program needn't handle non-finite values.
Results may differ from the reference program's by a relative error of at most 0.0073.
Values may be sent and summed in bfloat16 or wider, within the bound.
A program may use at most 64 MiB of HBM per device.

```python
import jax
import jax.numpy as jnp
from jax import lax

D = 4096
HEADS = 16
HEAD = 128
BLOCK = 64
SEQS = 2
LEN = 6144


def draw_tokens(key, part):
    key_base, key_level, key_common = jax.random.split(key, 3)
    blocks = LEN // BLOCK
    base_draw = jax.random.truncated_normal(key_base, -4.0, 4.0, (SEQS, LEN, D), jnp.float32)
    level_log = jax.random.uniform(key_level, (SEQS, blocks, 1, 1), jnp.float32, -1.0, 1.0)
    common = jnp.zeros((1, 1, D), jnp.float32)
    row_scale = jnp.broadcast_to(jnp.exp(level_log), (SEQS, blocks, BLOCK, 1)).reshape(SEQS, LEN, 1)
    return ((base_draw + common) * row_scale).astype(jnp.bfloat16)


def draw_rate_log(key, part):
    key_slow, key_quick, key_pick = jax.random.split(key, 3)
    slow_rates = jnp.log(jax.random.uniform(key_slow, (HEADS,), jnp.float32, 0.2, 0.6) / LEN)
    quick_rates = jnp.log(jax.random.uniform(key_quick, (HEADS,), jnp.float32, 0.02, 0.06))
    slow_picks = jax.random.randint(key_pick, (HEADS,), 0, 2)
    return jnp.where(slow_picks == 1, slow_rates, quick_rates)


def block_scale(stream_key, shape, shards, low, largest):
    factor_of = 1.0
    for dim, shards_of in shards:
        heights = jax.random.uniform(jax.random.fold_in(jax.random.fold_in(stream_key, 6), dim), (shards_of,), jnp.float32, low / len(shards), largest / len(shards))
        factor_of = factor_of * jnp.repeat(jnp.exp(heights), shape[dim] // shards_of).reshape((-1,) + (1,) * (len(shape) - 1 - dim))
    return factor_of


def centred(key, shape, scale, reach, pieces=(), kind=jnp.bfloat16):
    array = scale * jax.random.normal(key, shape, jnp.float32)
    if pieces:
        array = array * block_scale(key, shape, pieces, -0.22, 0.18)
    return jnp.clip(array, -reach, reach).astype(kind)


def setup_inputs(seed: int = 0) -> dict:
    streams_of = jax.random.split(jax.random.key(seed), 16)
    return {
        "tokens": draw_tokens(jax.random.fold_in(streams_of[15], 71), 0),
        "query_weight": centred(streams_of[1], (D, HEADS * HEAD), D ** -0.5, 0.09375, ((1, 8),)),
        "key_weight": centred(streams_of[2], (D, HEADS * HEAD), D ** -0.5, 0.09375, ((1, 8),)),
        "value_weight": centred(streams_of[3], (D, HEADS * HEAD), D ** -0.5, 0.09375, ((1, 8),)),
        "gate_weight": centred(streams_of[4], (D, HEADS * HEAD), D ** -0.5, 0.09375, ((1, 8),)),
        "beta_weight": centred(streams_of[5], (D, HEADS), D ** -0.5, 0.09375, ((1, 8),)),
        "decay_weight": centred(streams_of[6], (D, HEADS), D ** -0.5, 0.09375, ((1, 8),)),
        "beta_bias": jnp.clip(-6.0 + 3.0 * jax.random.uniform(streams_of[7], (HEADS,), jnp.float32) ** block_scale(streams_of[7], (HEADS,), ((0, 8),), -0.2, 0.2), -6.0, -3.0),
        "rate_log": draw_rate_log(jax.random.fold_in(streams_of[15], 71), 0),
        "out_gain": jnp.clip(1.0 + 0.18 * jax.random.normal(streams_of[9], (HEAD,), jnp.float32), 0.1, 1.9),
        "new_query": centred(streams_of[10], (SEQS, HEADS, HEAD), 1.0, 6.0, ((1, 8),)),
        "new_key": centred(streams_of[11], (SEQS, HEADS, HEAD), 1.0, 6.0, ((1, 8),)),
        "new_value": centred(streams_of[12], (SEQS, HEADS, HEAD), 1.0, 6.0, ((1, 8),)),
        "new_beta": jnp.clip(0.1 + 0.79999997 * jax.random.uniform(streams_of[13], (SEQS, HEADS), jnp.float32) ** block_scale(streams_of[13], (SEQS, HEADS), ((1, 8),), -0.2, 0.2), 0.1, 0.9),
        "new_decay": jnp.clip(0.3 + 0.7 * jax.random.uniform(streams_of[14], (SEQS, HEADS), jnp.float32) ** block_scale(streams_of[14], (SEQS, HEADS), ((1, 8),), -0.2, 0.2), 0.3, 1.0),
    }


unit_floor = 1.0
norm_floor = 0.001
highest = lax.Precision.HIGHEST

def matmul(form, left, right):
    return jnp.einsum(form, left, right, precision=highest)

def unit_rows(values):
    return values * lax.rsqrt(lax.optimization_barrier(jnp.sum(values * values, axis=-1, keepdims=True)) + unit_floor)

def head_norm(values, out_gain):
    return values * lax.rsqrt(lax.optimization_barrier(jnp.mean(values * values, axis=-1, keepdims=True)) + norm_floor) * out_gain

def stored(values):
    return lax.optimization_barrier(values.astype(jnp.bfloat16)).astype(jnp.float32)

def unit_lower_inverse(lower_part):
    extent = lower_part.shape[-1]
    nilpotent = -lower_part
    inverse = jnp.eye(extent, dtype=jnp.float32) + nilpotent
    for _ in range(extent.bit_length() - 2):
        nilpotent = matmul('...ij,...jk->...ik', nilpotent, nilpotent)
        inverse = inverse + matmul('...ij,...jk->...ik', nilpotent, inverse)
    return inverse

def prepare(query_rows, key_rows, value_rows, beta_in, decay_in, beta_bias, rate_log, seq_count, length, head_count):
    extent = query_rows.shape[-1] // head_count
    blocks = length // BLOCK

    def by_head(values):
        shaped = values.reshape(seq_count, blocks, BLOCK, head_count, extent)
        return shaped.transpose(0, 3, 1, 2, 4).reshape(seq_count * head_count, blocks, BLOCK, extent)

    def by_scalar(values):
        shaped = values.reshape(seq_count, blocks, BLOCK, head_count)
        return shaped.transpose(0, 3, 1, 2).reshape(seq_count * head_count, blocks, BLOCK)
    queries = unit_rows(by_head(query_rows))
    key_unit = unit_rows(by_head(key_rows))
    values = by_head(value_rows)
    strength = by_scalar(jax.nn.sigmoid(beta_in + beta_bias))
    decays = by_scalar(-jnp.exp(rate_log) * jax.nn.softplus(decay_in))
    return (queries, key_unit, values, strength, decays)

def block_terms(queries, key_unit, values, strength, decays):
    extent = decays.shape[-1]
    cumulative = jnp.cumsum(decays, axis=-1)
    causal = jnp.tril(jnp.ones((extent, extent), bool))
    strict = jnp.tril(jnp.ones((extent, extent), bool), -1)
    spread = cumulative[..., :, None] - cumulative[..., None, :]
    weights = jnp.where(causal, jnp.exp(jnp.where(causal, spread, 0.0)), 0.0)
    key_beta = key_unit * strength[..., None]
    lower_part = jnp.where(strict, matmul('...td,...sd->...ts', key_beta, key_unit) * weights, 0.0)
    inverse = unit_lower_inverse(lower_part)
    update = matmul('...ts,...se->...te', inverse, values * strength[..., None])
    carry_w = matmul('...ts,...sd->...td', inverse, key_beta * jnp.exp(cumulative)[..., None])
    scores = matmul('...td,...sd->...ts', queries, key_unit) * weights
    query_decay = queries * jnp.exp(cumulative)[..., None]
    last_log = cumulative[..., -1]
    key_decay = key_unit * jnp.exp(last_log[..., None] - cumulative)[..., None]
    return (update, carry_w, query_decay, scores, key_decay, last_log)

def first_read(cache_whole, new_query, new_key, new_value, new_beta, new_decay, out_gain):
    seq_count, head_count, extent, _ = cache_whole.shape
    memory = lax.optimization_barrier(cache_whole).astype(jnp.float32)
    query_unit = unit_rows(new_query.astype(jnp.float32))
    key_unit = unit_rows(new_key.astype(jnp.float32))
    recall = matmul('shde,shd->she', memory, query_unit)
    retrieve = matmul('shde,shd->she', memory, key_unit)
    intersect = lax.optimization_barrier(jnp.sum(key_unit * query_unit, axis=-1))
    fresh_values = new_value.astype(jnp.float32) - new_decay[..., None] * retrieve
    read_heads = new_decay[..., None] * recall + (new_beta * intersect)[..., None] * fresh_values
    return head_norm(read_heads, out_gain).reshape(seq_count, head_count * extent)

def reference(tokens, query_weight, key_weight, value_weight, gate_weight, beta_weight, decay_weight, beta_bias, rate_log, out_gain, new_query, new_key, new_value, new_beta, new_decay):
    flat_rows = tokens.reshape(SEQS * LEN, D)

    def project(weight):
        return jnp.dot(flat_rows, weight, preferred_element_type=jnp.float32)
    query_rows = stored(project(query_weight))
    key_rows = stored(project(key_weight))
    value_rows = stored(project(value_weight))
    gate_rows = stored(project(gate_weight))
    beta_in = project(beta_weight)
    decay_in = project(decay_weight)
    prepared = prepare(query_rows, key_rows, value_rows, beta_in, decay_in, beta_bias, rate_log, SEQS, LEN, HEADS)
    block_data = block_terms(*prepared)

    def advance(state_now, inputs):
        update, carry_w, query_decay, scores, key_decay, last_log = inputs
        fresh_values = update - matmul('btd,bde->bte', carry_w, state_now)
        block_out = matmul('btd,bde->bte', query_decay, state_now) + matmul('bts,bse->bte', scores, fresh_values)
        state_next = state_now * jnp.exp(last_log)[:, None, None] + matmul('bsd,bse->bde', key_decay, fresh_values)
        return (state_next, block_out)
    inputs = tuple((jnp.moveaxis(member, 1, 0) for member in block_data))
    batch_size = SEQS * HEADS
    final_state, outputs = lax.scan(advance, jnp.zeros((batch_size, HEAD, HEAD), jnp.float32), inputs)
    heads_out = outputs.reshape(LEN // BLOCK, SEQS, HEADS, BLOCK, HEAD).transpose(1, 0, 3, 2, 4)
    heads_out = heads_out.reshape(SEQS, LEN, HEADS, HEAD)
    gate_values = gate_rows.reshape(SEQS, LEN, HEADS, HEAD)
    mixed_out = (head_norm(heads_out, out_gain) * jax.nn.silu(gate_values)).astype(jnp.bfloat16)
    mixed_out = mixed_out.reshape(SEQS, LEN, HEADS * HEAD)
    cache = final_state.reshape(SEQS, HEADS, HEAD, HEAD).astype(jnp.bfloat16)
    first_out = first_read(cache, new_query, new_key, new_value, new_beta, new_decay, out_gain)
    return (mixed_out, cache, first_out)
```

```python
import types

import jax
import jax.numpy as jnp
from jax import lax
from jax.experimental import pallas as pl
from jax.experimental.pallas import tpu as pltpu
from jax.sharding import PartitionSpec as P

unit_floor = 1.0
norm_floor = 0.001
highest = lax.Precision.HIGHEST
MESH = pl.DeviceIdType.MESH
PAD = 8
GROUP = 4
BLOCK = 64
f32 = jnp.float32
bf16 = jnp.bfloat16

NN = (((1,), (0,)), ((), ()))
NT = (((1,), (1,)), ((), ()))
TN = (((0,), (0,)), ((), ()))


def dot(left, right, dims=NN, precision=None):
    return lax.dot_general(left, right, dims, precision=precision, preferred_element_type=f32)


def half(values):
    return values.astype(bf16)


def unit_rows(values):
    return values * lax.rsqrt(jnp.sum(values * values, axis=-1, keepdims=True) + unit_floor)


def iota(shape, dim):
    return lax.broadcasted_iota(jnp.int32, shape, dim)


def unit_lower_inverses(blocks):
    size = blocks[0].shape[0]
    row, col = iota((size, size), 0), iota((size, size), 1)
    unit = jnp.where(row == col, 1.0, 0.0)
    pair = ((row >> 1) == (col >> 1)) & (row > col)
    inv = [unit - jnp.where(pair, b, 0.0) for b in blocks]
    level = 1
    while (1 << level) < size:
        mask = ((row >> (level + 1)) == (col >> (level + 1))) & ((row >> level) > (col >> level))
        inv_h = [half(m) for m in inv]
        mid = [half(dot(half(jnp.where(mask, b, 0.0)), m)) for b, m in zip(blocks, inv_h)]
        inv = [m - dot(mh, t) for m, mh, t in zip(inv, inv_h, mid)]
        level += 1
    return [half(m) for m in inv]


def fused_kernel(names, dims, *refs):
    r = types.SimpleNamespace(**dict(zip(names, refs)))
    seqs, heads, span, extent, kc = dims
    hv = extent // 2
    box = extent + hv
    nblk = span // BLOCK

    me = lax.axis_index("tp")
    y, c = me // 2, lax.rem(me, 2)
    sp = lax.axis_index("sp")
    z, x = sp // GROUP, lax.rem(sp, GROUP)
    zl = lax.rem(z, GROUP)
    lower_quad = z < GROUP
    partner = y * 2 + (1 - c)

    def tid(dy, core):
        return lax.rem(y + dy + 4, 4) * 2 + core

    nxt, prv, opp = tid(1, c), tid(-1, c), tid(2, c)
    order = [me, partner, prv, tid(-1, 1 - c), nxt, tid(1, 1 - c), opp, tid(2, 1 - c)]
    kd = 2 * kc
    weights = (r.wq, r.wk, r.wv, r.wg)

    def sp_id(zz, xx):
        return {"sp": zz * GROUP + xx}

    def peer_x(d):
        return lax.rem(x + d, GROUP)

    def peer_zl(d):
        return lax.rem(zl + d, GROUP)

    def peer_z(d):
        return z - zl + peer_zl(d)

    barrier = pltpu.get_barrier_semaphore()

    def greet(device):
        pl.semaphore_signal(barrier, inc=1, device_id=device, device_id_type=MESH)

    for t in (nxt, prv, partner):
        greet({"tp": t})
    for d in range(1, GROUP):
        greet(sp_id(z, peer_x(d)))
        greet(sp_id(peer_z(d), x))

    is_a, is_b = z == GROUP - 1, z == 0
    spreads = jnp.logical_or(is_a, is_b)

    def spread_to(k):
        return jnp.where(is_a, GROUP + k, 2 * GROUP - 1 - k)

    @pl.when(spreads)
    def _():
        for k in range(2):
            greet(sp_id(spread_to(k), x))

    spread_from = jnp.where(z < GROUP + 2, GROUP - 1, 0)

    @pl.when(jnp.logical_not(lower_quad))
    def _():
        greet(sp_id(spread_from, x))

    def token_copy(s, hf):
        return pltpu.make_async_copy(
            r.x.at[s, :, pl.ds(hf * kc, kc)], r.xs.at[me, s, hf], r.tok_sem.at[s, hf]
        )

    for s in range(seqs):
        for hf in range(2):
            token_copy(s, hf).start()

    def weight_copy(w, slot):
        start = pl.multiple_of(order[slot] * kd, kd)
        return pltpu.make_async_copy(weights[w].at[pl.ds(start, kd), :], r.wbuf.at[w, slot], r.wsem.at[w, slot])

    for slot in range(8):
        for w in range(4):
            weight_copy(w, slot).start()
    r.bd[...] = jnp.zeros_like(r.bd)
    r.bd[0:heads] = r.bw[...]
    r.bd[PAD : PAD + heads] = r.dw[...]
    extra = jnp.where(spreads, 2, jnp.where(lower_quad, 0, 1))
    pl.semaphore_wait(barrier, 3 + 2 * (GROUP - 1) + extra)

    def ring(b, s, hf, to, sem):
        return pltpu.make_async_remote_copy(
            src_ref=r.xs.at[b, s, hf], dst_ref=r.xs.at[b, s, hf], send_sem=sem,
            recv_sem=r.rx.at[b, s, hf], device_id={"tp": to}, device_id_type=MESH,
        )

    def own_sends(s):
        return [
            ring(me, s, 0, nxt, r.own_sem.at[0, s, 0]),
            ring(me, s, 1, prv, r.own_sem.at[1, s, 1]),
            ring(me, s, 1, nxt, r.own_sem.at[0, s, 1]),
            ring(me, s, 0, prv, r.own_sem.at[1, s, 0]),
            ring(me, s, 0, partner, r.part_sem.at[0, s, 0]),
            ring(me, s, 1, partner, r.part_sem.at[0, s, 1]),
        ]

    def forward(s, i):
        return ring((prv, nxt)[i], s, i, (nxt, prv)[i], r.fwd_sem.at[i, s])

    def partner_send(s, i, hf):
        return ring((prv, nxt, opp)[i], s, hf, partner, r.part_sem.at[1 + i, s, hf])

    def arrive(b, s, hf):
        ring(b, s, hf, partner, r.part_sem.at[0, s, hf]).wait_recv()

    def use(s, items, first=False):
        parts = [r.xs[order[slot], s, hf] for slot, hf in items]
        if s == 0:
            for slot in sorted({slot for slot, hf in items} - set(waited)):
                waited.append(slot)
                for w in range(4):
                    weight_copy(w, slot).wait()
        for w in range(4):
            total = None
            for (slot, hf), part in zip(items, parts):
                term = dot(part, r.wbuf[w, slot, hf * kc : (hf + 1) * kc, :])
                total = term if total is None else total + term
            r.acc[w] = total if first else r.acc[w] + total
        total = None
        for (slot, hf), part in zip(items, parts):
            piece = r.bd[:, pl.ds(pl.multiple_of(order[slot] * kd + hf * kc, kc), kc)]
            term = dot(piece, part, NT)
            total = term if total is None else total + term
        r.sacc[...] = total if first else r.sacc[...] + total

    waited = []

    def start_own(s):
        for hf in range(2):
            token_copy(s, hf).wait()
        for copy in own_sends(s):
            copy.start()

    def first_arrivals(s):
        arrive(prv, s, 0)
        forward(s, 0).start()
        arrive(nxt, s, 1)
        forward(s, 1).start()
        partner_send(s, 0, 0).start()
        partner_send(s, 1, 1).start()

    def rest(s):
        arrive(order[3], s, 0)
        arrive(order[5], s, 1)
        use(s, [(3, 0), (5, 1)])
        arrive(prv, s, 1)
        partner_send(s, 0, 1).start()
        arrive(nxt, s, 0)
        partner_send(s, 1, 0).start()
        use(s, [(2, 1), (4, 0)])
        arrive(order[3], s, 1)
        arrive(order[5], s, 0)
        use(s, [(3, 1), (5, 0)])
        arrive(opp, s, 0)
        partner_send(s, 2, 0).start()
        arrive(opp, s, 1)
        partner_send(s, 2, 1).start()
        use(s, [(6, 0), (6, 1)])
        arrive(order[7], s, 0)
        arrive(order[7], s, 1)
        use(s, [(7, 0), (7, 1)])
        for w in range(4):
            r.rows[s, w] = half(r.acc[w])

    def near(s):
        use(s, [(0, 0), (0, 1)], True)
        for hf in range(2):
            arrive(partner, s, hf)
        use(s, [(1, 0), (1, 1)])


    slot_of = iota((PAD, 1), 0)
    bias = jnp.zeros((PAD, 1), f32)
    rate = jnp.zeros((PAD, 1), f32)
    for h in range(heads):
        bias = jnp.where(slot_of == h, r.bias[h], bias)
        rate = jnp.where(slot_of == h, r.rate[h], rate)

    def x_copy(s, o):
        return pltpu.make_async_remote_copy(
            src_ref=r.out1.at[s, o], dst_ref=r.in1.at[s, x], send_sem=r.send1.at[s, o],
            recv_sem=r.recv1.at[s, x], device_id=sp_id(z, o), device_id_type=MESH,
        )

    def local(s, hook):
        upper = jnp.where(iota((span, span), 0) <= iota((span, span), 1), 1.0, 0.0)
        beta8 = jax.nn.sigmoid(r.sacc[0:PAD] + bias)
        pre = r.sacc[PAD : 2 * PAD]
        soft = jnp.maximum(pre, 0.0) + jnp.log1p(jnp.exp(-jnp.abs(pre)))
        cum8 = dot(-jnp.exp(rate) * soft, upper, NN, highest)
        cum_t, beta_t = cum8.T, beta8.T
        row, col = iota((BLOCK, BLOCK), 0), iota((BLOCK, BLOCK), 1)
        causal = row >= col
        per_head = []
        diags = []
        for h in range(heads):
            lanes = slice(h * extent, (h + 1) * extent)
            q = unit_rows(r.rows[s, 0, :, lanes].astype(f32))
            k = unit_rows(r.rows[s, 1, :, lanes].astype(f32))
            v = r.rows[s, 2, :, lanes].astype(f32)
            cumc, beta = cum_t[:, h : h + 1], beta_t[:, h : h + 1]
            cumr = cum8[h : h + 1, :]
            kb = k * beta
            qh, kh, kbh = half(q), half(k), half(kb)
            grow = jnp.exp(cumc)
            last = cumc[span - 1 :, :]
            right = jnp.concatenate([v * beta, kb * grow], axis=1)
            low_off, sc_diag, sc_off = [], [], []
            for i in range(nblk):
                at = slice(i * BLOCK, (i + 1) * BLOCK)
                diff = cumc[at] - cumr[:, at]
                w_d = jnp.where(causal, jnp.exp(jnp.where(causal, diff, 0.0)), 0.0)
                diags.append(jnp.where(row > col, dot(kbh[at], kh[at], NT) * w_d, 0.0))
                sc_diag.append(half(dot(qh[at], kh[at], NT) * w_d))
                if i:
                    before = slice(0, i * BLOCK)
                    w_o = jnp.exp(cumc[at] - cumr[:, before])
                    low_off.append(half(dot(kbh[at], kh[before], NT) * w_o))
                    sc_off.append(half(dot(qh[at], kh[before], NT) * w_o))
            per_head.append(
                dict(right=right, low=low_off, scd=sc_diag, sco=sc_off, qg=q * grow, last=last,
                     kdec=half(k * jnp.exp(last - cumc)))
            )
        hook()
        inv = unit_lower_inverses(diags)
        done = [[] for _ in range(heads)]
        for i in range(nblk):
            at = slice(i * BLOCK, (i + 1) * BLOCK)
            for h in range(heads):
                e = per_head[h]
                rhs = e["right"][at]
                if i:
                    rhs = rhs - dot(e["low"][i - 1], jnp.concatenate(done[h], axis=0) if i > 1 else done[h][0])
                done[h].append(half(dot(inv[h * nblk + i], half(rhs))))
        eye = iota((extent, extent), 0) == iota((extent, extent), 1)
        for h in range(heads):
            e = per_head[h]
            uw = jnp.concatenate(done[h], axis=0)
            fin = dot(uw, e["kdec"], TN)
            step = half(jnp.where(eye, jnp.exp(e["last"]) - 1.0, 0.0) - fin[extent:])
            state = half(fin[:extent])
            for f in range(2):
                r.out1[s, 2 * h + f, 0:extent, :] = step
                r.out1[s, 2 * h + f, extent:, :] = state[f * hv : (f + 1) * hv]
        for o in range(GROUP):

            @pl.when(x != o)
            def _():
                x_copy(s, o).start()

            @pl.when(x == o)
            def _():
                r.in1[s, x] = r.out1[s, o]

        for h in range(heads):
            e = per_head[h]
            for i in range(nblk):
                at = slice(i * BLOCK, (i + 1) * BLOCK)
                out = dot(e["scd"][i], done[h][i])
                if i:
                    out = out + dot(e["sco"][i - 1], jnp.concatenate(done[h][:i], axis=0) if i > 1 else done[h][0])
                r.local_out[s, h, at, :] = out[:, :extent]
                r.reach[s, h, at, :] = half(e["qg"][at] - out[:, extent:])
            gate = r.rows[s, 3, :, h * extent : (h + 1) * extent].astype(f32)
            r.gated[s, h] = gate * jax.nn.sigmoid(gate) * r.gain[...]


    def compose(prefix, step):
        e = step[0:extent]
        return prefix + dot(half(prefix), e) + step.astype(f32)

    def quad_copy(s, d):
        return pltpu.make_async_remote_copy(
            src_ref=r.in2.at[s, zl], dst_ref=r.in2.at[s, zl], send_sem=r.send2.at[s, d - 1],
            recv_sem=r.recv2.at[s, zl], device_id=sp_id(peer_z(d), x), device_id_type=MESH,
        )

    def combine_group(s):
        for j in range(GROUP):

            @pl.when(x != j)
            def _():
                pltpu.make_async_remote_copy(
                    src_ref=r.out1.at[s, 0], dst_ref=r.in1.at[s, j], send_sem=r.send1.at[s, 0],
                    recv_sem=r.recv1.at[s, j], device_id=sp_id(z, j), device_id_type=MESH,
                ).wait_recv()

        prefix = r.in1[s, 0].astype(f32)
        for j in range(1, GROUP):
            r.gpre[s, j - 1] = prefix
            prefix = compose(prefix, r.in1[s, j])
        r.in2[s, zl] = half(prefix)
        for d in (3, 2, 1):
            quad_copy(s, d).start()

    def spread_copy(s, k):
        return pltpu.make_async_remote_copy(
            src_ref=r.s4_out.at[s], dst_ref=r.s4_in.at[s], send_sem=r.send3.at[s, k],
            recv_sem=r.recv3.at[s], device_id=sp_id(spread_to(k), x), device_id_type=MESH,
        )

    def state_copy(s, xx):
        return pltpu.make_async_remote_copy(
            src_ref=r.st_out.at[s, xx], dst_ref=r.st_in.at[s, x], send_sem=r.send4.at[s, xx],
            recv_sem=r.recv4.at[s, x], device_id=sp_id(z, xx), device_id_type=MESH,
        )

    def give_states(s, states):
        for xx in range(GROUP):
            r.st_out[s, xx] = half(states[xx])
        for xx in range(GROUP):

            @pl.when(x != xx)
            def _():
                state_copy(s, xx).start()

            @pl.when(x == xx)
            def _():
                r.st_in[s, x] = r.st_out[s, xx]

    def combine_quad(s):
        for d in range(1, GROUP):
            j = peer_zl(d)
            pltpu.make_async_remote_copy(
                src_ref=r.in2.at[s, j], dst_ref=r.in2.at[s, j], send_sem=r.send2.at[s, 0],
                recv_sem=r.recv2.at[s, j], device_id=sp_id(peer_z(d), x), device_id_type=MESH,
            ).wait_recv()
        r.qpre[0] = jnp.zeros((box, extent), f32)
        prefix = r.in2[s, 0].astype(f32)
        r.qpre[1] = prefix
        for j in range(1, GROUP):
            prefix = compose(prefix, r.in2[s, j])
            if j < GROUP - 1:
                r.qpre[j + 1] = prefix
        r.qtot[s] = prefix

        @pl.when(spreads)
        def _():
            r.s4_out[s] = half(prefix[extent:])
            for k in range(2):
                spread_copy(s, k).start()

        mine = r.qpre[zl]
        mine_h = half(mine)
        comps = [mine]
        for j in range(1, GROUP):
            g = r.gpre[s, j - 1]
            comps.append(mine + dot(mine_h, half(g[0:extent])) + g)

        @pl.when(lower_quad)
        def _():
            give_states(s, [m[extent:] for m in comps])

        @pl.when(jnp.logical_not(lower_quad))
        def _():
            for j in range(GROUP):
                r.comp_d[s, j] = half(comps[j][0:extent])
                r.comp_c[s, j] = comps[j][extent:]

    tails = jnp.logical_or(z == GROUP, z == 2 * GROUP - 1)

    def tail_z(i):
        return jnp.where(z == GROUP, 2 + i, lax.rem(6 + i, 2 * GROUP))

    def tail_copy(s, i, xx):
        return pltpu.make_async_remote_copy(
            src_ref=r.tail_out.at[s, i * GROUP + xx], dst_ref=r.tail_in.at[s, x],
            send_sem=r.send_t.at[s, i * GROUP + xx], recv_sem=r.recv_t.at[s, x],
            device_id=sp_id(tail_z(i), xx), device_id_type=MESH,
        )

    def tail_self(i, xx):
        return jnp.logical_and(tail_z(i) == z, x == xx)

    def tail(s, s4, s4h):
        tot = r.qtot[s]
        memory = half(s4 + dot(s4h, half(tot[0:extent])) + tot[extent:]).astype(f32)
        shape = r.nq.shape
        mine = (iota(shape, 0) == s) & (iota(shape, 1) == x // 2)

        def own(ref):
            kept = jnp.where(mine, ref[...].astype(f32), 0.0)
            return jnp.sum(jnp.sum(kept, axis=0), axis=0, keepdims=True)

        qn, kn = unit_rows(own(r.nq)), unit_rows(own(r.nk))
        both = jnp.concatenate(
            [jnp.broadcast_to(qn, (PAD, extent)), jnp.broadcast_to(kn, (PAD, extent))], axis=0
        )
        twice = jnp.concatenate([memory, memory], axis=0)
        reads = dot(both, twice, NT, highest)
        recall, retrieve = reads[0:1], reads[PAD : PAD + 1]
        beta_new, decay_new = r.nb[s, x // 2], r.nd[s, x // 2]
        fresh = own(r.nv) - decay_new * retrieve
        meet = jnp.sum(kn * qn, axis=-1, keepdims=True)
        kept = (iota((1, extent), 1) // hv) == lax.rem(x, 2)
        read = jnp.where(kept, decay_new * recall + (beta_new * meet) * fresh, 0.0)
        r.memt[...] = jnp.where(kept, twice.T, 0.0)
        answer = jnp.broadcast_to(read, (4, extent))
        for i in range(GROUP):
            base = pl.multiple_of(tail_z(i) * 16, 16)
            keys = r.memt[pl.ds(base, 16), :]
            for xx in range(GROUP):
                r.tail_out[s, i * GROUP + xx, 0:4] = keys[xx * 4 : xx * 4 + 4]
                r.tail_out[s, i * GROUP + xx, 4:8] = answer
        for i in range(GROUP):
            for xx in range(GROUP):

                @pl.when(tail_self(i, xx))
                def _():
                    r.tail_in[s, x] = r.tail_out[s, i * GROUP + xx]

                @pl.when(jnp.logical_not(tail_self(i, xx)))
                def _():
                    tail_copy(s, i, xx).start()

    def upper(s):
        @pl.when(jnp.logical_not(lower_quad))
        def _():
            pltpu.make_async_remote_copy(
                src_ref=r.s4_out.at[s], dst_ref=r.s4_in.at[s], send_sem=r.send3.at[s, 0],
                recv_sem=r.recv3.at[s], device_id=sp_id(spread_from, x), device_id_type=MESH,
            ).wait_recv()
            s4h = r.s4_in[s]
            s4 = s4h.astype(f32)
            give_states(s, [s4 + dot(s4h, r.comp_d[s, j]) + r.comp_c[s, j] for j in range(GROUP)])

            @pl.when(tails)
            def _():
                tail(s, s4, s4h)

    def finish(s):
        for o in range(GROUP):

            @pl.when(x != o)
            def _():
                pltpu.make_async_remote_copy(
                    src_ref=r.st_out.at[s, 0], dst_ref=r.st_in.at[s, o], send_sem=r.send4.at[s, 0],
                    recv_sem=r.recv4.at[s, o], device_id=sp_id(z, o), device_id_type=MESH,
                ).wait_recv()

        for h in range(heads):
            state_t = jnp.concatenate([r.st_in[s, 2 * h], r.st_in[s, 2 * h + 1]], axis=0)
            o = r.local_out[s, h] + dot(r.reach[s, h], state_t, NT)
            norm = lax.rsqrt(jnp.mean(o * o, axis=-1, keepdims=True) + norm_floor)
            r.mixed[s, :, h * extent : (h + 1) * extent] = half(o * norm * r.gated[s, h])

    def last_read(s):
        from_z = jnp.where((z >= 2) & (z < 6), GROUP, 2 * GROUP - 1)
        for o in range(GROUP):

            @pl.when(jnp.logical_not((z == from_z) & (x == o)))
            def _():
                pltpu.make_async_remote_copy(
                    src_ref=r.tail_out.at[s, 0], dst_ref=r.tail_in.at[s, o], send_sem=r.send_t.at[s, 0],
                    recv_sem=r.recv_t.at[s, o], device_id=sp_id(from_z, o), device_id_type=MESH,
                ).wait_recv()

        for h in range(heads):
            both = r.tail_in[s, 2 * h] + r.tail_in[s, 2 * h + 1]
            r.cache[s, h] = half(both[0:4])
            read = both[4:5]
            norm = lax.rsqrt(jnp.mean(read * read, axis=-1, keepdims=True) + norm_floor)
            r.first[s : s + 1, h * extent : (h + 1) * extent] = read * norm * r.gain[...]

    start_own(0)
    near(0)
    first_arrivals(0)
    start_own(1)
    use(0, [(2, 0), (4, 1)])
    rest(0)
    local(0, lambda: first_arrivals(1))
    near(1)
    use(1, [(2, 0), (4, 1)])
    rest(1)
    local(1, lambda: None)
    combine_group(0)
    combine_group(1)
    combine_quad(0)
    upper(0)
    finish(0)
    combine_quad(1)
    upper(1)
    finish(1)
    last_read(0)
    last_read(1)

    for s in range(seqs):
        for copy in own_sends(s):
            copy.wait_send()
        for i in range(2):
            forward(s, i).wait_send()
        for i in range(3):
            for hf in range(2):
                partner_send(s, i, hf).wait_send()
        for o in range(GROUP):

            @pl.when(x != o)
            def _():
                x_copy(s, o).wait_send()
                state_copy(s, o).wait_send()

        for d in range(1, GROUP):
            quad_copy(s, d).wait_send()

        @pl.when(spreads)
        def _():
            for k in range(2):
                spread_copy(s, k).wait_send()

        @pl.when(tails)
        def _():
            for i in range(GROUP):
                for xx in range(GROUP):

                    @pl.when(jnp.logical_not(tail_self(i, xx)))
                    def _():
                        tail_copy(s, i, xx).wait_send()


def shards(
    tokens, query_weight, key_weight, value_weight, gate_weight, beta_weight, decay_weight,
    beta_bias, rate_log, out_gain, new_query, new_key, new_value, new_beta, new_decay,
):
    seqs, span, kd = tokens.shape
    heads = rate_log.shape[0]
    extent = out_gain.shape[0]
    depth, width = query_weight.shape
    kc = kd // 2
    hv, box = extent // 2, extent + extent // 2
    key_rows = extent // lax.axis_size("sp")
    vmem = pl.BlockSpec(memory_space=pltpu.VMEM)
    smem = pl.BlockSpec(memory_space=pltpu.SMEM)
    hbm = pl.BlockSpec(memory_space=pl.ANY)
    inputs = dict(
        x=hbm, wq=hbm, wk=hbm, wv=hbm, wg=hbm, bw=vmem, dw=vmem, bias=smem, rate=smem, gain=vmem,
        nq=vmem, nk=vmem, nv=vmem, nb=smem, nd=smem,
    )
    outputs = dict(
        mixed=jax.ShapeDtypeStruct((seqs, span, width), bf16),
        cache=jax.ShapeDtypeStruct((seqs, heads, key_rows, extent), bf16),
        first=jax.ShapeDtypeStruct((seqs, width), f32),
    )
    dma = pltpu.SemaphoreType.DMA
    scratch = dict(
        bd=pltpu.VMEM((2 * PAD, depth), bf16),
        xs=pltpu.VMEM((8, seqs, 2, span, kc), bf16),
        wbuf=pltpu.VMEM((4, 8, kd, width), bf16),
        acc=pltpu.VMEM((4, span, width), f32),
        sacc=pltpu.VMEM((2 * PAD, span), f32),
        rows=pltpu.VMEM((seqs, 4, span, width), bf16),
        local_out=pltpu.VMEM((seqs, heads, span, extent), f32),
        reach=pltpu.VMEM((seqs, heads, span, extent), bf16),
        gated=pltpu.VMEM((seqs, heads, span, extent), f32),
        out1=pltpu.VMEM((seqs, GROUP, box, extent), bf16),
        in1=pltpu.VMEM((seqs, GROUP, box, extent), bf16),
        gpre=pltpu.VMEM((seqs, GROUP - 1, box, extent), f32),
        in2=pltpu.VMEM((seqs, GROUP, box, extent), bf16),
        qpre=pltpu.VMEM((GROUP, box, extent), f32),
        qtot=pltpu.VMEM((seqs, box, extent), f32),
        comp_d=pltpu.VMEM((seqs, GROUP, extent, extent), bf16),
        comp_c=pltpu.VMEM((seqs, GROUP, hv, extent), f32),
        s4_out=pltpu.VMEM((seqs, hv, extent), bf16),
        s4_in=pltpu.VMEM((seqs, hv, extent), bf16),
        st_out=pltpu.VMEM((seqs, GROUP, hv, extent), bf16),
        st_in=pltpu.VMEM((seqs, GROUP, hv, extent), bf16),
        memt=pltpu.VMEM((extent, extent), f32),
        tail_out=pltpu.VMEM((seqs, GROUP * GROUP, PAD, extent), f32),
        tail_in=pltpu.VMEM((seqs, GROUP, PAD, extent), f32),
        tok_sem=dma((seqs, 2)),
        wsem=dma((4, 8)),
        own_sem=dma((2, seqs, 2)),
        fwd_sem=dma((2, seqs)),
        part_sem=dma((4, seqs, 2)),
        rx=dma((8, seqs, 2)),
        send1=dma((seqs, GROUP)),
        recv1=dma((seqs, GROUP)),
        send2=dma((seqs, GROUP)),
        recv2=dma((seqs, GROUP)),
        send3=dma((seqs, 2)),
        recv3=dma((seqs,)),
        send4=dma((seqs, GROUP)),
        recv4=dma((seqs, GROUP)),
        send_t=dma((seqs, GROUP * GROUP)),
        recv_t=dma((seqs, GROUP)),
    )
    names = list(inputs) + list(outputs) + list(scratch)
    dims = (seqs, heads, span, extent, kc)

    def body(*refs):
        fused_kernel(names, dims, *refs)

    return pl.pallas_call(
        body,
        out_shape=tuple(outputs.values()),
        in_specs=list(inputs.values()),
        out_specs=(vmem,) * 3,
        scratch_shapes=list(scratch.values()),
        compiler_params=pltpu.CompilerParams(
            collective_id=0, has_side_effects=True, vmem_limit_bytes=60 * 1024 * 1024
        ),
        name="fused",
    )(
        tokens, query_weight, key_weight, value_weight, gate_weight, beta_weight.T, decay_weight.T,
        beta_bias, rate_log, out_gain[None], new_query, new_key, new_value, new_beta, new_decay,
    )


def solution(mesh):
    placed = (
        P(None, "sp", "tp"),
        P(None, "tp"),
        P(None, "tp"),
        P(None, "tp"),
        P(None, "tp"),
        P(None, "tp"),
        P(None, "tp"),
        P("tp"),
        P("tp"),
        P(),
        P(None, "tp", None),
        P(None, "tp", None),
        P(None, "tp", None),
        P(None, "tp"),
        P(None, "tp"),
    )
    return jax.shard_map(
        shards,
        mesh=mesh,
        in_specs=placed,
        out_specs=(P(None, "sp", "tp"), P(None, "tp", "sp", None), P(None, "tp")),
        check_vma=False,
    )
```

```python
import types

import jax
import jax.numpy as jnp
from jax import lax
from jax.experimental import pallas as pl
from jax.experimental.pallas import tpu as pltpu
from jax.sharding import PartitionSpec as P

unit_floor = 1.0
norm_floor = 0.001
highest = lax.Precision.HIGHEST
MESH = pl.DeviceIdType.MESH
PAD = 8
GROUP = 4
BLOCK = 64
SMALL = ("bw", "dw", "bias", "rate", "gain", "nq", "nk", "nv", "nb", "nd")
f32 = jnp.float32
bf16 = jnp.bfloat16

NN = (((1,), (0,)), ((), ()))
NT = (((1,), (1,)), ((), ()))
TN = (((0,), (0,)), ((), ()))


def dot(left, right, dims=NN, precision=None):
    return lax.dot_general(left, right, dims, precision=precision, preferred_element_type=f32)


def half(values):
    return values.astype(bf16)


def unit_rows(values):
    return values * lax.rsqrt(jnp.sum(values * values, axis=-1, keepdims=True) + unit_floor)


def iota(shape, dim):
    return lax.broadcasted_iota(jnp.int32, shape, dim)


def unit_lower_inverses(blocks):
    size = blocks[0].shape[0]
    row, col = iota((size, size), 0), iota((size, size), 1)
    unit = jnp.where(row == col, 1.0, 0.0)
    pair = ((row >> 1) == (col >> 1)) & (row > col)
    inv = [unit - jnp.where(pair, b, 0.0) for b in blocks]
    level = 1
    while (1 << level) < size:
        mask = ((row >> (level + 1)) == (col >> (level + 1))) & ((row >> level) > (col >> level))
        inv_h = [half(m) for m in inv]
        mid = [half(dot(half(jnp.where(mask, b, 0.0)), m)) for b, m in zip(blocks, inv_h)]
        inv = [m - dot(mh, t) for m, mh, t in zip(inv, inv_h, mid)]
        level += 1
    return [half(m) for m in inv]


def fused_kernel(names, dims, *refs):
    r = types.SimpleNamespace(**dict(zip(names, refs)))
    seqs, heads, span, extent, kc = dims
    hv = extent // 2
    box = extent + hv
    nblk = span // BLOCK

    me = lax.axis_index("tp")
    y, c = me // 2, lax.rem(me, 2)
    sp = lax.axis_index("sp")
    z, x = sp // GROUP, lax.rem(sp, GROUP)
    zl = lax.rem(z, GROUP)
    lower_quad = z < GROUP
    partner = y * 2 + (1 - c)

    def tid(dy, core):
        return lax.rem(y + dy + 4, 4) * 2 + core

    nxt, prv, opp = tid(1, c), tid(-1, c), tid(2, c)
    order = [me, partner, prv, tid(-1, 1 - c), nxt, tid(1, 1 - c), opp, tid(2, 1 - c)]
    kd = 2 * kc
    weights = (r.wq, r.wk, r.wv, r.wg)

    def sp_id(zz, xx):
        return {"sp": zz * GROUP + xx}

    def peer_x(d):
        return lax.rem(x + d, GROUP)

    barrier = pltpu.get_barrier_semaphore()

    def greet(device):
        pl.semaphore_signal(barrier, inc=1, device_id=device, device_id_type=MESH)

    x_near = [sp_id(z, peer_x(d)) for d in (1, 3)]
    z_near = [sp_id(lax.rem(z + d, 2 * GROUP), x) for d in (1, 2 * GROUP - 1)]
    near_ones = [{"tp": t} for t in (nxt, prv, partner)] + x_near + z_near
    for device in near_ones:
        greet(device)

    def relay(devices, sem):
        for device in devices:
            pl.semaphore_signal(sem, inc=1, device_id=device, device_id_type=MESH)

    is_a, is_b = z == GROUP - 1, z == 0
    spreads = jnp.logical_or(is_a, is_b)

    def spread_to(k):
        return jnp.where(is_a, GROUP + k, 2 * GROUP - 1 - k)

    spread_from = jnp.where(z < GROUP + 2, GROUP - 1, 0)

    def rows_of(s):
        return pl.ds(s * span, span)

    def token_copy(s, hf):
        return pltpu.make_async_copy(
            r.x.at[s, :, pl.ds(hf * kc, kc)], r.xs.at[me, hf, rows_of(s)], r.tok_sem.at[s, hf]
        )

    for s in range(seqs):
        for hf in range(2):
            token_copy(s, hf).start()

    def weight_copy(w, slot):
        start = pl.multiple_of(order[slot] * kd, kd)
        return pltpu.make_async_copy(weights[w].at[pl.ds(start, kd), :], r.wbuf.at[w, slot], r.wsem.at[w, slot])

    def small_copy(name):
        return pltpu.make_async_copy(
            getattr(r, name + "_hbm"), getattr(r, name), r.small_sem.at[SMALL.index(name)]
        )

    for slot in range(8):
        for w in range(4):
            weight_copy(w, slot).start()
    for name in SMALL:
        small_copy(name).start()
    r.bd[...] = jnp.zeros_like(r.bd)
    pl.semaphore_wait(barrier, len(near_ones))

    def ring(b, s, hf, to, sem):
        return pltpu.make_async_remote_copy(
            src_ref=r.xs.at[b, hf, rows_of(s)], dst_ref=r.xs.at[b, hf, rows_of(s)], send_sem=sem,
            recv_sem=r.rx.at[b, s, hf], device_id={"tp": to}, device_id_type=MESH,
        )

    def own_send(s, i, step):
        hf = i if step == 0 else 1 - i
        return ring(me, s, hf, (nxt, prv)[i], r.own_sem.at[i, s, hf])

    def own_partner(s, hf):
        return ring(me, s, hf, partner, r.part_sem.at[0, s, hf])

    def start_own(s, step):
        for i in range(2):
            own_send(s, i, step).start()

    def forward(s, i):
        return ring((prv, nxt)[i], s, i, (nxt, prv)[i], r.fwd_sem.at[i, s])

    def partner_send(s, i, hf):
        return ring((prv, nxt, opp)[i], s, hf, partner, r.part_sem.at[1 + i, s, hf])

    def arrive(b, s, hf):
        ring(b, s, hf, partner, r.part_sem.at[0, s, hf]).wait_recv()

    def use(seq_list, items, first=False):
        at = pl.ds(seq_list[0] * span, len(seq_list) * span)
        parts = [r.xs[order[slot], hf, at] for slot, hf in items]
        for slot in sorted({slot for slot, hf in items} - set(waited)):
            waited.append(slot)
            for w in range(4):
                weight_copy(w, slot).wait()
        for w in range(4):
            total = None
            for (slot, hf), part in zip(items, parts):
                term = dot(part, r.wbuf[w, slot, hf * kc : (hf + 1) * kc, :])
                total = term if total is None else total + term
            r.acc[w, at] = total if first else r.acc[w, at] + total
        for i, s in enumerate(seq_list):
            total = None
            for (slot, hf), part in zip(items, parts):
                piece = r.bd[:, pl.ds(pl.multiple_of(order[slot] * kd + hf * kc, kc), kc)]
                term = dot(piece, part[i * span : (i + 1) * span], NT)
                total = term if total is None else total + term
            r.sacc[s] = total if first else r.sacc[s] + total

    waited = []
    both = list(range(seqs))

    def begin():
        for hf in range(2):
            token_copy(0, hf).wait()
        for step in range(2):
            start_own(0, step)
        for hf in range(2):
            own_partner(0, hf).start()
        for s in range(1, seqs):
            for hf in range(2):
                token_copy(s, hf).wait()
                own_partner(s, hf).start()
        relay(x_near, r.relay_x)
        relay(z_near, r.relay_z.at[0])
        for name in SMALL:
            small_copy(name).wait()
        r.bd[0:heads] = r.bw[...]
        r.bd[PAD : PAD + heads] = r.dw[...]

    def near():
        use(both, [(0, 0), (0, 1)], True)
        for s in both:
            for hf in range(2):
                arrive(partner, s, hf)
        use(both, [(1, 0), (1, 1)])
        pl.semaphore_wait(r.relay_x, 2)
        pl.semaphore_wait(r.relay_z.at[0], 2)
        relay(z_near, r.relay_z.at[1])

    def near_first(s):
        arrive(prv, s, 0)
        forward(s, 0).start()
        partner_send(s, 0, 0).start()
        arrive(nxt, s, 1)
        forward(s, 1).start()
        partner_send(s, 1, 1).start()

    def near_second(s):
        arrive(prv, s, 1)
        partner_send(s, 0, 1).start()
        arrive(nxt, s, 0)
        partner_send(s, 1, 0).start()

    def far(s):
        for hf in range(2):
            arrive(opp, s, hf)
            partner_send(s, 2, hf).start()

    def cross_first(s):
        arrive(order[3], s, 0)
        arrive(order[5], s, 1)

    def cross_second(s):
        arrive(order[3], s, 1)
        arrive(order[5], s, 0)

    def cross_far(s):
        for hf in range(2):
            arrive(order[7], s, hf)

    def round_rows(s):
        for w in range(4):
            r.rows[s, w] = half(r.acc[w, rows_of(s)])


    def x_copy(s, o):
        return pltpu.make_async_remote_copy(
            src_ref=r.out1.at[s, o], dst_ref=r.in1.at[s, x], send_sem=r.send1.at[s, o],
            recv_sem=r.recv1.at[s, x], device_id=sp_id(z, o), device_id_type=MESH,
        )

    def local(s, hook, hook2):
        slot_of = iota((PAD, 1), 0)
        bias = jnp.zeros((PAD, 1), f32)
        rate = jnp.zeros((PAD, 1), f32)
        for h in range(heads):
            bias = jnp.where(slot_of == h, r.bias[h], bias)
            rate = jnp.where(slot_of == h, r.rate[h], rate)
        upper = jnp.where(iota((span, span), 0) <= iota((span, span), 1), 1.0, 0.0)
        beta8 = jax.nn.sigmoid(r.sacc[s, 0:PAD] + bias)
        pre = r.sacc[s, PAD : 2 * PAD]
        soft = jnp.maximum(pre, 0.0) + jnp.log1p(jnp.exp(-jnp.abs(pre)))
        cum8 = dot(-jnp.exp(rate) * soft, upper, NN, highest)
        cum_t, beta_t = cum8.T, beta8.T
        row, col = iota((BLOCK, BLOCK), 0), iota((BLOCK, BLOCK), 1)
        causal = row >= col
        per_head = []
        diags = []
        for h in range(heads):
            lanes = slice(h * extent, (h + 1) * extent)
            q = unit_rows(r.rows[s, 0, :, lanes].astype(f32))
            k = unit_rows(r.rows[s, 1, :, lanes].astype(f32))
            v = r.rows[s, 2, :, lanes].astype(f32)
            cumc, beta = cum_t[:, h : h + 1], beta_t[:, h : h + 1]
            cumr = cum8[h : h + 1, :]
            kb = k * beta
            qh, kh, kbh = half(q), half(k), half(kb)
            grow = jnp.exp(cumc)
            last = cumc[span - 1 :, :]
            right = jnp.concatenate([v * beta, kb * grow], axis=1)
            low_off, sc_diag, sc_off = [], [], []
            for i in range(nblk):
                at = slice(i * BLOCK, (i + 1) * BLOCK)
                diff = cumc[at] - cumr[:, at]
                w_d = jnp.where(causal, jnp.exp(jnp.where(causal, diff, 0.0)), 0.0)
                diags.append(jnp.where(row > col, dot(kbh[at], kh[at], NT) * w_d, 0.0))
                sc_diag.append(half(dot(qh[at], kh[at], NT) * w_d))
                if i:
                    before = slice(0, i * BLOCK)
                    w_o = jnp.exp(cumc[at] - cumr[:, before])
                    low_off.append(half(dot(kbh[at], kh[before], NT) * w_o))
                    sc_off.append(half(dot(qh[at], kh[before], NT) * w_o))
            per_head.append(
                dict(right=right, low=low_off, scd=sc_diag, sco=sc_off, qg=q * grow, last=last,
                     kdec=half(k * jnp.exp(last - cumc)))
            )
        hook()
        inv = unit_lower_inverses(diags)
        hook2()
        done = [[] for _ in range(heads)]
        for i in range(nblk):
            at = slice(i * BLOCK, (i + 1) * BLOCK)
            for h in range(heads):
                e = per_head[h]
                rhs = e["right"][at]
                if i:
                    rhs = rhs - dot(e["low"][i - 1], jnp.concatenate(done[h], axis=0) if i > 1 else done[h][0])
                done[h].append(half(dot(inv[h * nblk + i], half(rhs))))
        eye = iota((extent, extent), 0) == iota((extent, extent), 1)
        for h in range(heads):
            e = per_head[h]
            uw = jnp.concatenate(done[h], axis=0)
            fin = dot(uw, e["kdec"], TN)
            step = half(jnp.where(eye, jnp.exp(e["last"]) - 1.0, 0.0) - fin[extent:])
            state = half(fin[:extent])
            for f in range(2):
                r.out1[s, 2 * h + f, 0:extent, :] = step
                r.out1[s, 2 * h + f, extent:, :] = state[f * hv : (f + 1) * hv]
        for d in (2, 1, 3):
            x_copy(s, peer_x(d)).start()
        r.in1[s, x] = r.out1[s, x]

        for h in range(heads):
            e = per_head[h]
            for i in range(nblk):
                at = slice(i * BLOCK, (i + 1) * BLOCK)
                out = dot(e["scd"][i], done[h][i])
                if i:
                    out = out + dot(e["sco"][i - 1], jnp.concatenate(done[h][:i], axis=0) if i > 1 else done[h][0])
                r.local_out[s, h, at, :] = out[:, :extent]
                r.reach[s, h, at, :] = half(e["qg"][at] - out[:, extent:])
            gate = r.rows[s, 3, :, h * extent : (h + 1) * extent].astype(f32)
            r.gated[s, h] = gate * jax.nn.sigmoid(gate) * r.gain[...]


    def compose(prefix, step):
        e = step[0:extent]
        return prefix + dot(half(prefix), e) + step.astype(f32)

    def quad_copy(s, j, source, part):
        return pltpu.make_async_remote_copy(
            src_ref=r.in2.at[s, source, part], dst_ref=r.in2.at[s, source, part],
            send_sem=r.send2.at[s, j], recv_sem=r.recv2.at[s, source],
            device_id=sp_id(z - zl + j, x), device_id_type=MESH,
        )

    whole, state_only = pl.ds(0, box), pl.ds(extent, hv)

    def quad_each(s, act):
        for j in (3, 2, 1, 0):
            if j:

                @pl.when(is_b)
                def _():
                    act(quad_copy(s, j, zl, state_only))

                @pl.when(jnp.logical_and(zl < j, jnp.logical_not(is_b)))
                def _():
                    act(quad_copy(s, j, zl, whole))
            else:

                @pl.when(zl > 0)
                def _():
                    act(quad_copy(s, 0, zl, whole))

    def quad_arrive(s, j):
        if j == 0:

            @pl.when(jnp.logical_and(zl > 0, lower_quad))
            def _():
                quad_copy(s, 0, 0, state_only).wait_recv()

            @pl.when(jnp.logical_and(zl > 0, jnp.logical_not(lower_quad)))
            def _():
                quad_copy(s, 0, 0, whole).wait_recv()
        else:

            @pl.when(jnp.logical_or(zl > j, zl == 0))
            def _():
                quad_copy(s, 0, j, whole).wait_recv()

    def combine_group(s):
        for j in range(GROUP):

            @pl.when(x != j)
            def _():
                pltpu.make_async_remote_copy(
                    src_ref=r.out1.at[s, 0], dst_ref=r.in1.at[s, j], send_sem=r.send1.at[s, 0],
                    recv_sem=r.recv1.at[s, j], device_id=sp_id(z, j), device_id_type=MESH,
                ).wait_recv()

        prefix = r.in1[s, 0].astype(f32)
        for j in range(1, GROUP):
            r.gpre[s, j - 1] = prefix
            prefix = compose(prefix, r.in1[s, j])
        r.in2[s, zl] = half(prefix)
        quad_each(s, lambda copy: copy.start())

    def spread_copy(s, k):
        return pltpu.make_async_remote_copy(
            src_ref=r.s4_out.at[s], dst_ref=r.s4_in.at[s], send_sem=r.send3.at[s, k],
            recv_sem=r.recv3.at[s], device_id=sp_id(spread_to(k), x), device_id_type=MESH,
        )

    def state_copy(s, xx):
        return pltpu.make_async_remote_copy(
            src_ref=r.st_out.at[s, xx], dst_ref=r.st_in.at[s, x], send_sem=r.send4.at[s, xx],
            recv_sem=r.recv4.at[s, x], device_id=sp_id(z, xx), device_id_type=MESH,
        )

    def give_states(s, states):
        for xx in range(GROUP):
            r.st_out[s, xx] = half(states[xx])
        for d in (2, 1, 3):
            state_copy(s, peer_x(d)).start()
        r.st_in[s, x] = r.st_out[s, x]

    def with_groups(mine, mine_h, take, s):
        comps = [mine]
        for j in range(1, GROUP):
            g = r.gpre[s, j - 1]
            comps.append(mine + dot(mine_h, half(g[0:extent])) + g[take])
        return comps

    def combine_lower(s):
        r.qs[0] = jnp.zeros((hv, extent), f32)

        def give():
            mine = r.qs[zl]
            give_states(s, with_groups(mine, half(mine), slice(extent, box), s))

        @pl.when(is_b)
        def _():
            give()

        for j in range(GROUP):

            @pl.when(jnp.logical_or(zl > j, spreads))
            def _():
                quad_arrive(s, j)
                step = r.in2[s, j, extent:].astype(f32)
                if j:
                    state = r.qs[j]
                    step = state + dot(half(state), r.in2[s, j, 0:extent]) + step
                r.qs[j + 1] = step

        @pl.when(spreads)
        def _():
            r.s4_out[s] = half(r.qs[GROUP])
            for k in range(2):
                spread_copy(s, k).start()

        @pl.when(jnp.logical_not(is_b))
        def _():
            give()

    ends = jnp.logical_or(zl == 0, zl == GROUP - 1)

    def combine_upper(s):
        r.qpre[0] = jnp.zeros((box, extent), f32)
        for j in range(GROUP):

            @pl.when(jnp.logical_or(zl > j, ends))
            def _():
                quad_arrive(s, j)
                got = r.in2[s, j]
                r.qpre[j + 1] = got.astype(f32) if j == 0 else compose(r.qpre[j], got)

        @pl.when(ends)
        def _():
            r.qtot[s] = r.qpre[GROUP]

        mine = r.qpre[zl]
        comps = with_groups(mine, half(mine), slice(0, box), s)
        for j in range(GROUP):
            r.comp_d[s, j] = half(comps[j][0:extent])
            r.comp_c[s, j] = comps[j][extent:]

    def combine_quad(s):
        @pl.when(lower_quad)
        def _():
            combine_lower(s)

        @pl.when(jnp.logical_not(lower_quad))
        def _():
            combine_upper(s)

    tails = jnp.logical_or(z == GROUP, z == 2 * GROUP - 1)

    def tail_z(i):
        return jnp.where(z == GROUP, 2 + i, lax.rem(6 + i, 2 * GROUP))

    def tail_copy(s, i, xx):
        return pltpu.make_async_remote_copy(
            src_ref=r.tail_out.at[s, i * GROUP + xx], dst_ref=r.tail_in.at[s, x],
            send_sem=r.send_t.at[s, i * GROUP + xx], recv_sem=r.recv_t.at[s, x],
            device_id=sp_id(tail_z(i), xx), device_id_type=MESH,
        )

    def tail_self(i, xx):
        return jnp.logical_and(tail_z(i) == z, x == xx)

    def prepare_read(s):
        shape = r.nq.shape
        mine = (iota(shape, 0) == s) & (iota(shape, 1) == x // 2)

        def own(ref):
            kept = jnp.where(mine, ref[...].astype(f32), 0.0)
            return jnp.sum(jnp.sum(kept, axis=0), axis=0, keepdims=True)

        qn, kn = unit_rows(own(r.nq)), unit_rows(own(r.nk))
        r.pair_row[s, 0:1] = own(r.nv)
        r.pair_row[s, 1:2] = jnp.broadcast_to(jnp.sum(kn * qn, axis=-1, keepdims=True), (1, extent))
        for i, row in enumerate((qn, kn)):
            r.pair_col[s, i] = jnp.broadcast_to(row, (extent, extent)).T

    def tail(s, s4, s4h):
        tot = r.qtot[s]
        memory = half(s4 + dot(s4h, half(tot[0:extent])) + tot[extent:]).astype(f32)
        twice = jnp.concatenate([memory, memory], axis=0).T
        recall = jnp.sum(twice * r.pair_col[s, 0], axis=0, keepdims=True)
        retrieve = jnp.sum(twice * r.pair_col[s, 1], axis=0, keepdims=True)
        beta_new, decay_new = r.nb[s, x // 2], r.nd[s, x // 2]
        fresh = r.pair_row[s, 0:1] - decay_new * retrieve
        kept = (iota((1, extent), 1) // hv) == lax.rem(x, 2)
        read = jnp.where(kept, decay_new * recall + (beta_new * r.pair_row[s, 1:2]) * fresh, 0.0)
        r.memt[...] = jnp.where(kept, twice, 0.0)
        answer = jnp.broadcast_to(read, (4, extent))
        for i in range(GROUP):
            base = pl.multiple_of(tail_z(i) * 16, 16)
            keys = r.memt[pl.ds(base, 16), :]
            for xx in range(GROUP):
                r.tail_out[s, i * GROUP + xx, 0:4] = keys[xx * 4 : xx * 4 + 4]
                r.tail_out[s, i * GROUP + xx, 4:8] = answer
        for i in range(GROUP):
            for xx in range(GROUP):

                @pl.when(tail_self(i, xx))
                def _():
                    r.tail_in[s, x] = r.tail_out[s, i * GROUP + xx]

                @pl.when(jnp.logical_not(tail_self(i, xx)))
                def _():
                    tail_copy(s, i, xx).start()

    def upper(s):
        @pl.when(jnp.logical_not(lower_quad))
        def _():
            pltpu.make_async_remote_copy(
                src_ref=r.s4_out.at[s], dst_ref=r.s4_in.at[s], send_sem=r.send3.at[s, 0],
                recv_sem=r.recv3.at[s], device_id=sp_id(spread_from, x), device_id_type=MESH,
            ).wait_recv()
            s4h = r.s4_in[s]
            s4 = s4h.astype(f32)
            give_states(s, [s4 + dot(s4h, r.comp_d[s, j]) + r.comp_c[s, j] for j in range(GROUP)])

            @pl.when(tails)
            def _():
                tail(s, s4, s4h)

    def finish(s):
        for o in range(GROUP):

            @pl.when(x != o)
            def _():
                pltpu.make_async_remote_copy(
                    src_ref=r.st_out.at[s, 0], dst_ref=r.st_in.at[s, o], send_sem=r.send4.at[s, 0],
                    recv_sem=r.recv4.at[s, o], device_id=sp_id(z, o), device_id_type=MESH,
                ).wait_recv()

        for h in range(heads):
            state_t = jnp.concatenate([r.st_in[s, 2 * h], r.st_in[s, 2 * h + 1]], axis=0)
            o = r.local_out[s, h] + dot(r.reach[s, h], state_t, NT)
            norm = lax.rsqrt(jnp.mean(o * o, axis=-1, keepdims=True) + norm_floor)
            r.mixed[s, :, h * extent : (h + 1) * extent] = half(o * norm * r.gated[s, h])

    def last_read(s):
        from_z = jnp.where((z >= 2) & (z < 6), GROUP, 2 * GROUP - 1)
        for o in range(GROUP):

            @pl.when(jnp.logical_not((z == from_z) & (x == o)))
            def _():
                pltpu.make_async_remote_copy(
                    src_ref=r.tail_out.at[s, 0], dst_ref=r.tail_in.at[s, o], send_sem=r.send_t.at[s, 0],
                    recv_sem=r.recv_t.at[s, o], device_id=sp_id(from_z, o), device_id_type=MESH,
                ).wait_recv()

        for h in range(heads):
            both = r.tail_in[s, 2 * h] + r.tail_in[s, 2 * h + 1]
            r.cache[s, h] = half(both[0:4])
            read = both[4:5]
            norm = lax.rsqrt(jnp.mean(read * read, axis=-1, keepdims=True) + norm_floor)
            r.first[s : s + 1, h * extent : (h + 1) * extent] = read * norm * r.gain[...]

    def phase(name, step, *args):
        with jax.named_scope(name):
            step(*args)

    def group0_early():
        pl.semaphore_wait(r.relay_z.at[1], 2)
        phase("group0", combine_group, 0)

    phase("begin", begin)
    phase("near", near)
    phase("nf0", near_first, 0)
    phase("u0a", use, [0], [(2, 0), (4, 1)])
    phase("ns0", near_second, 0)
    phase("own1a", start_own, 1, 0)
    phase("cf0", cross_first, 0)
    phase("u0b", use, [0], [(3, 0), (5, 1), (2, 1), (4, 0)])
    phase("far0", far, 0)
    phase("own1b", start_own, 1, 1)
    phase("cs0", cross_second, 0)
    phase("u0c", use, [0], [(3, 1), (5, 0), (6, 0), (6, 1)])
    phase("cfar0", cross_far, 0)
    phase("u0d", use, [0], [(7, 0), (7, 1)])
    phase("rows0", round_rows, 0)
    phase("local0", local, 0, lambda: phase("nf1", near_first, 1), lambda: phase("ns1", near_second, 1))
    phase("u1a", use, [1], [(2, 0), (4, 1), (2, 1), (4, 0)])
    phase("far1", far, 1)
    phase("cc1", cross_first, 1)
    phase("cs1", cross_second, 1)
    phase("u1b", use, [1], [(3, 0), (5, 1), (3, 1), (5, 0)])
    phase("u1c", use, [1], [(6, 0), (6, 1)])
    phase("cfar1", cross_far, 1)
    phase("u1d", use, [1], [(7, 0), (7, 1)])
    phase("rows1", round_rows, 1)
    phase("local1", local, 1, group0_early, lambda: None)
    for s in range(seqs):
        phase(f"prep{s}", prepare_read, s)
    phase("group1", combine_group, 1)
    phase("quad0", combine_quad, 0)
    phase("upper0", upper, 0)
    phase("quad1", combine_quad, 1)
    phase("finish0", finish, 0)
    phase("upper1", upper, 1)
    phase("finish1", finish, 1)
    phase("read0", last_read, 0)
    phase("read1", last_read, 1)

    for s in range(seqs):
        for i in range(2):
            own_partner(s, i).wait_send()
            forward(s, i).wait_send()
            for step in range(2):
                own_send(s, i, step).wait_send()
        for i in range(3):
            for hf in range(2):
                partner_send(s, i, hf).wait_send()
        for d in range(1, GROUP):
            x_copy(s, peer_x(d)).wait_send()
            state_copy(s, peer_x(d)).wait_send()
        quad_each(s, lambda copy: copy.wait_send())

        @pl.when(spreads)
        def _():
            for k in range(2):
                spread_copy(s, k).wait_send()

        @pl.when(tails)
        def _():
            for i in range(GROUP):
                for xx in range(GROUP):

                    @pl.when(jnp.logical_not(tail_self(i, xx)))
                    def _():
                        tail_copy(s, i, xx).wait_send()


def shards(
    tokens, query_weight, key_weight, value_weight, gate_weight, beta_weight, decay_weight,
    beta_bias, rate_log, out_gain, new_query, new_key, new_value, new_beta, new_decay,
):
    seqs, span, kd = tokens.shape
    heads = rate_log.shape[0]
    extent = out_gain.shape[0]
    depth, width = query_weight.shape
    kc = kd // 2
    hv, box = extent // 2, extent + extent // 2
    key_rows = extent // lax.axis_size("sp")
    vmem = pl.BlockSpec(memory_space=pltpu.VMEM)
    hbm = pl.BlockSpec(memory_space=pltpu.HBM)
    inputs = ["x", "wq", "wk", "wv", "wg"] + [n + "_hbm" for n in SMALL]
    outputs = dict(
        mixed=jax.ShapeDtypeStruct((seqs, span, width), bf16),
        cache=jax.ShapeDtypeStruct((seqs, heads, key_rows, extent), bf16),
        first=jax.ShapeDtypeStruct((seqs, width), f32),
    )
    dma = pltpu.SemaphoreType.DMA
    scratch = dict(
        bw=pltpu.VMEM((heads, depth), bf16),
        dw=pltpu.VMEM((heads, depth), bf16),
        bias=pltpu.SMEM((heads,), f32),
        rate=pltpu.SMEM((heads,), f32),
        gain=pltpu.VMEM((1, extent), f32),
        nq=pltpu.VMEM((seqs, heads, extent), bf16),
        nk=pltpu.VMEM((seqs, heads, extent), bf16),
        nv=pltpu.VMEM((seqs, heads, extent), bf16),
        nb=pltpu.SMEM((seqs, heads), f32),
        nd=pltpu.SMEM((seqs, heads), f32),
        small_sem=dma((len(SMALL),)),
        bd=pltpu.VMEM((2 * PAD, depth), bf16),
        xs=pltpu.VMEM((8, 2, seqs * span, kc), bf16),
        wbuf=pltpu.VMEM((4, 8, kd, width), bf16),
        acc=pltpu.VMEM((4, seqs * span, width), f32),
        sacc=pltpu.VMEM((seqs, 2 * PAD, span), f32),
        rows=pltpu.VMEM((seqs, 4, span, width), bf16),
        local_out=pltpu.VMEM((seqs, heads, span, extent), f32),
        reach=pltpu.VMEM((seqs, heads, span, extent), bf16),
        gated=pltpu.VMEM((seqs, heads, span, extent), f32),
        out1=pltpu.VMEM((seqs, GROUP, box, extent), bf16),
        in1=pltpu.VMEM((seqs, GROUP, box, extent), bf16),
        gpre=pltpu.VMEM((seqs, GROUP - 1, box, extent), f32),
        in2=pltpu.VMEM((seqs, GROUP, box, extent), bf16),
        qpre=pltpu.VMEM((GROUP + 1, box, extent), f32),
        qs=pltpu.VMEM((GROUP + 1, hv, extent), f32),
        pair_row=pltpu.VMEM((seqs, PAD, extent), f32),
        pair_col=pltpu.VMEM((seqs, 2, extent, extent), f32),
        relay_x=pltpu.SemaphoreType.REGULAR,
        relay_z=pltpu.SemaphoreType.REGULAR((2,)),
        qtot=pltpu.VMEM((seqs, box, extent), f32),
        comp_d=pltpu.VMEM((seqs, GROUP, extent, extent), bf16),
        comp_c=pltpu.VMEM((seqs, GROUP, hv, extent), f32),
        s4_out=pltpu.VMEM((seqs, hv, extent), bf16),
        s4_in=pltpu.VMEM((seqs, hv, extent), bf16),
        st_out=pltpu.VMEM((seqs, GROUP, hv, extent), bf16),
        st_in=pltpu.VMEM((seqs, GROUP, hv, extent), bf16),
        memt=pltpu.VMEM((extent, extent), f32),
        tail_out=pltpu.VMEM((seqs, GROUP * GROUP, PAD, extent), f32),
        tail_in=pltpu.VMEM((seqs, GROUP, PAD, extent), f32),
        tok_sem=dma((seqs, 2)),
        wsem=dma((4, 8)),
        own_sem=dma((2, seqs, 2)),
        fwd_sem=dma((2, seqs)),
        part_sem=dma((4, seqs, 2)),
        rx=dma((8, seqs, 2)),
        send1=dma((seqs, GROUP)),
        recv1=dma((seqs, GROUP)),
        send2=dma((seqs, GROUP)),
        recv2=dma((seqs, GROUP)),
        send3=dma((seqs, 2)),
        recv3=dma((seqs,)),
        send4=dma((seqs, GROUP)),
        recv4=dma((seqs, GROUP)),
        send_t=dma((seqs, GROUP * GROUP)),
        recv_t=dma((seqs, GROUP)),
    )
    names = inputs + list(outputs) + list(scratch)
    dims = (seqs, heads, span, extent, kc)

    def body(*refs):
        fused_kernel(names, dims, *refs)

    return pl.pallas_call(
        body,
        out_shape=tuple(outputs.values()),
        in_specs=[hbm] * len(inputs),
        out_specs=(vmem,) * 3,
        scratch_shapes=list(scratch.values()),
        compiler_params=pltpu.CompilerParams(
            collective_id=0, has_side_effects=True, vmem_limit_bytes=32 * 1024 * 1024
        ),
        name="fused",
    )(
        *(
            pltpu.with_memory_space_constraint(value, pltpu.HBM)
            for value in (
                tokens, query_weight, key_weight, value_weight, gate_weight, beta_weight.T, decay_weight.T,
                beta_bias, rate_log, out_gain[None], new_query, new_key, new_value, new_beta, new_decay,
            )
        )
    )


def solution(mesh):
    placed = (
        P(None, "sp", "tp"),
        P(None, "tp"),
        P(None, "tp"),
        P(None, "tp"),
        P(None, "tp"),
        P(None, "tp"),
        P(None, "tp"),
        P("tp"),
        P("tp"),
        P(),
        P(None, "tp", None),
        P(None, "tp", None),
        P(None, "tp", None),
        P(None, "tp"),
        P(None, "tp"),
    )
    return jax.shard_map(
        shards,
        mesh=mesh,
        in_specs=placed,
        out_specs=(P(None, "sp", "tp"), P(None, "tp", "sp", None), P(None, "tp")),
        check_vma=False,
    )
```

```python
import types

import jax
import jax.numpy as jnp
from jax import lax
from jax.experimental import pallas as pl
from jax.experimental.pallas import tpu as pltpu
from jax.sharding import PartitionSpec as P

unit_floor = 1.0
norm_floor = 0.001
highest = lax.Precision.HIGHEST
MESH = pl.DeviceIdType.MESH
PAD = 8
GROUP = 4
BLOCK = 64
SMALL = ("bw", "dw", "bias", "rate", "gain", "nq", "nk", "nv", "nb", "nd")
f32 = jnp.float32
bf16 = jnp.bfloat16

NN = (((1,), (0,)), ((), ()))
NT = (((1,), (1,)), ((), ()))
TN = (((0,), (0,)), ((), ()))


def dot(left, right, dims=NN, precision=None):
    return lax.dot_general(left, right, dims, precision=precision, preferred_element_type=f32)


def half(values):
    return values.astype(bf16)


def unit_rows(values):
    return values * lax.rsqrt(jnp.sum(values * values, axis=-1, keepdims=True) + unit_floor)


def iota(shape, dim):
    return lax.broadcasted_iota(jnp.int32, shape, dim)


def unit_lower_inverses(blocks):
    size = blocks[0].shape[0]
    row, col = iota((size, size), 0), iota((size, size), 1)
    unit = jnp.where(row == col, 1.0, 0.0)
    four = ((row >> 2) == (col >> 2)) & (row > col)
    low = [jnp.where(four, b, 0.0) for b in blocks]
    low_h = [half(g) for g in low]
    square = [dot(g, g) for g in low_h]
    inv = [unit - g + q - dot(half(q), gh) for g, gh, q in zip(low, low_h, square)]
    level = 2
    while (1 << level) < size:
        mask = ((row >> (level + 2)) == (col >> (level + 2))) & ((row >> level) > (col >> level))
        t = [half(m) for m in inv]
        g = [dot(th, half(jnp.where(mask, b, 0.0))) for th, b in zip(t, blocks)]
        gh = [half(m) for m in g]
        first = [dot(m, th) for m, th in zip(gh, t)]
        second = [dot(m, m) for m in gh]
        inv = [
            m - f + dot(half(gg - q), half(f)) for m, f, gg, q in zip(inv, first, g, second)
        ]
        level += 2
    return [half(m) for m in inv]


def fused_kernel(names, dims, *refs):
    r = types.SimpleNamespace(**dict(zip(names, refs)))
    seqs, heads, span, extent, kc = dims
    hv = extent // 2
    box = extent + hv
    nblk = span // BLOCK

    me = lax.axis_index("tp")
    y, c = me // 2, lax.rem(me, 2)
    sp = lax.axis_index("sp")
    z, x = sp // GROUP, lax.rem(sp, GROUP)
    zl = lax.rem(z, GROUP)
    lower_quad = z < GROUP
    partner = y * 2 + (1 - c)

    def tid(dy, core):
        return lax.rem(y + dy + 4, 4) * 2 + core

    nxt, prv, opp = tid(1, c), tid(-1, c), tid(2, c)
    order = [me, partner, prv, tid(-1, 1 - c), nxt, tid(1, 1 - c), opp, tid(2, 1 - c)]
    kd = 2 * kc
    weights = (r.wq, r.wk, r.wv, r.wg)

    def sp_id(zz, xx):
        return {"sp": zz * GROUP + xx}

    def peer_x(d):
        return lax.rem(x + d, GROUP)

    barrier = pltpu.get_barrier_semaphore()

    def greet(device):
        pl.semaphore_signal(barrier, inc=1, device_id=device, device_id_type=MESH)

    x_near = [sp_id(z, peer_x(d)) for d in (1, 3)]
    z_near = [sp_id(lax.rem(z + d, 2 * GROUP), x) for d in (1, 2 * GROUP - 1)]
    near_ones = [{"tp": t} for t in (nxt, prv, partner)] + x_near + z_near
    for device in near_ones:
        greet(device)

    def relay(devices, sem):
        for device in devices:
            pl.semaphore_signal(sem, inc=1, device_id=device, device_id_type=MESH)

    is_a, is_b = z == GROUP - 1, z == 0
    spreads = jnp.logical_or(is_a, is_b)

    def spread_to(k):
        return jnp.where(is_a, GROUP + k, 2 * GROUP - 1 - k)

    spread_from = jnp.where(z < GROUP + 2, GROUP - 1, 0)

    def rows_of(s):
        return pl.ds(s * span, span)

    def token_copy(s, hf):
        return pltpu.make_async_copy(
            r.x.at[s, :, pl.ds(hf * kc, kc)], r.xs.at[me, hf, rows_of(s)], r.tok_sem.at[s, hf]
        )

    for s in range(seqs):
        for hf in range(2):
            token_copy(s, hf).start()

    def weight_copy(w, slot):
        start = pl.multiple_of(order[slot] * kd, kd)
        return pltpu.make_async_copy(weights[w].at[pl.ds(start, kd), :], r.wbuf.at[w, slot], r.wsem.at[w, slot])

    def small_copy(name):
        return pltpu.make_async_copy(
            getattr(r, name + "_hbm"), getattr(r, name), r.small_sem.at[SMALL.index(name)]
        )

    for name in SMALL:
        small_copy(name).start()
    for slot in range(8):
        for w in range(4):
            weight_copy(w, slot).start()
    r.bd[...] = jnp.zeros_like(r.bd)
    pl.semaphore_wait(barrier, len(near_ones))

    def ring(b, s, hf, to, sem):
        return pltpu.make_async_remote_copy(
            src_ref=r.xs.at[b, hf, rows_of(s)], dst_ref=r.xs.at[b, hf, rows_of(s)], send_sem=sem,
            recv_sem=r.rx.at[b, s, hf], device_id={"tp": to}, device_id_type=MESH,
        )

    def own_send(s, i, step):
        hf = i if step == 0 else 1 - i
        return ring(me, s, hf, (nxt, prv)[i], r.own_sem.at[i, s, hf])

    def own_partner(s, hf):
        return ring(me, s, hf, partner, r.part_sem.at[0, s, hf])

    def start_own(s, step):
        for i in range(2):
            own_send(s, i, step).start()

    def forward(s, i):
        return ring((prv, nxt)[i], s, i, (nxt, prv)[i], r.fwd_sem.at[i, s])

    def partner_send(s, i, hf):
        return ring((prv, nxt, opp)[i], s, hf, partner, r.part_sem.at[1 + i, s, hf])

    def arrive(b, s, hf):
        ring(b, s, hf, partner, r.part_sem.at[0, s, hf]).wait_recv()

    def use(seq_list, items, first=False):
        at = pl.ds(seq_list[0] * span, len(seq_list) * span)
        parts = [r.xs[order[slot], hf, at] for slot, hf in items]
        for slot in sorted({slot for slot, hf in items} - set(waited)):
            waited.append(slot)
            for w in range(4):
                weight_copy(w, slot).wait()
        for w in range(4):
            total = None
            for (slot, hf), part in zip(items, parts):
                term = dot(part, r.wbuf[w, slot, hf * kc : (hf + 1) * kc, :])
                total = term if total is None else total + term
            r.acc[w, at] = total if first else r.acc[w, at] + total
        for i, s in enumerate(seq_list):
            total = None
            for (slot, hf), part in zip(items, parts):
                piece = r.bd[:, pl.ds(pl.multiple_of(order[slot] * kd + hf * kc, kc), kc)]
                term = dot(piece, part[i * span : (i + 1) * span], NT)
                total = term if total is None else total + term
            r.sacc[s] = total if first else r.sacc[s] + total

    waited = []
    both = list(range(seqs))

    def begin():
        for hf in range(2):
            token_copy(0, hf).wait()
        for step in range(2):
            start_own(0, step)
        for hf in range(2):
            own_partner(0, hf).start()
        for s in range(1, seqs):
            for hf in range(2):
                token_copy(s, hf).wait()
                own_partner(s, hf).start()
        relay(x_near, r.relay_x)
        relay(z_near, r.relay_z.at[0])
        for name in SMALL:
            small_copy(name).wait()
        r.bd[0:heads] = r.bw[...]
        r.bd[PAD : PAD + heads] = r.dw[...]

    def near():
        use(both, [(0, 0), (0, 1)], True)
        for s in both:
            for hf in range(2):
                arrive(partner, s, hf)
        use(both, [(1, 0), (1, 1)])
        pl.semaphore_wait(r.relay_x, 2)
        pl.semaphore_wait(r.relay_z.at[0], 2)
        relay(z_near, r.relay_z.at[1])

    def near_first(s):
        arrive(prv, s, 0)
        forward(s, 0).start()
        partner_send(s, 0, 0).start()
        arrive(nxt, s, 1)
        forward(s, 1).start()
        partner_send(s, 1, 1).start()

    def near_second(s):
        arrive(prv, s, 1)
        partner_send(s, 0, 1).start()
        arrive(nxt, s, 0)
        partner_send(s, 1, 0).start()

    def far(s):
        for hf in range(2):
            arrive(opp, s, hf)
            partner_send(s, 2, hf).start()

    def cross_first(s):
        arrive(order[3], s, 0)
        arrive(order[5], s, 1)

    def cross_second(s):
        arrive(order[3], s, 1)
        arrive(order[5], s, 0)

    def cross_far(s):
        for hf in range(2):
            arrive(order[7], s, hf)

    def round_rows(s):
        for w in range(4):
            r.rows[s, w] = half(r.acc[w, rows_of(s)])


    def x_copy(s, o):
        return pltpu.make_async_remote_copy(
            src_ref=r.out1.at[s, o], dst_ref=r.in1.at[s, x], send_sem=r.send1.at[s, o],
            recv_sem=r.recv1.at[s, x], device_id=sp_id(z, o), device_id_type=MESH,
        )

    def local(s, hook, after):
        slot_of = iota((PAD, 1), 0)
        bias = jnp.zeros((PAD, 1), f32)
        rate = jnp.zeros((PAD, 1), f32)
        for h in range(heads):
            bias = jnp.where(slot_of == h, r.bias[h], bias)
            rate = jnp.where(slot_of == h, r.rate[h], rate)
        upper = half(jnp.where(iota((span, span), 0) <= iota((span, span), 1), 1.0, 0.0))
        beta8 = jax.nn.sigmoid(r.sacc[s, 0:PAD] + bias)
        pre = r.sacc[s, PAD : 2 * PAD]
        soft = jnp.maximum(pre, 0.0) + jnp.log1p(jnp.exp(-jnp.abs(pre)))
        decay = -jnp.exp(rate) * soft
        high = half(decay).astype(f32)
        mid = half(decay - high).astype(f32)
        thirds = dot(half(jnp.concatenate([high, mid, decay - high - mid], axis=0)), upper)
        cum8 = thirds[0:PAD] + thirds[PAD : 2 * PAD] + thirds[2 * PAD :]
        cum_t, beta_t = cum8.T, beta8.T
        r.cum_row[s] = cum8
        r.cum_col[s] = cum_t
        row, col = iota((BLOCK, BLOCK), 0), iota((BLOCK, BLOCK), 1)
        causal = row >= col
        per_head = []
        diags = []
        for h in range(heads):
            lanes = slice(h * extent, (h + 1) * extent)
            k = unit_rows(r.rows[s, 1, :, lanes].astype(f32))
            v = r.rows[s, 2, :, lanes].astype(f32)
            cumc, beta = cum_t[:, h : h + 1], beta_t[:, h : h + 1]
            cumr = cum8[h : h + 1, :]
            kb = k * beta
            kh, kbh = half(k), half(kb)
            grow = jnp.exp(cumc)
            last = cumc[span - 1 :, :]
            right = jnp.concatenate([v * beta, kb * grow], axis=1)
            low_off = []
            for i in range(nblk):
                at = slice(i * BLOCK, (i + 1) * BLOCK)
                diff = cumc[at] - cumr[:, at]
                w_d = jnp.where(causal, jnp.exp(jnp.where(causal, diff, 0.0)), 0.0)
                diags.append(jnp.where(row > col, dot(kbh[at], kh[at], NT) * w_d, 0.0))
                if i:
                    before = slice(0, i * BLOCK)
                    w_o = jnp.exp(cumc[at] - cumr[:, before])
                    low_off.append(half(dot(kbh[at], kh[before], NT) * w_o))
            per_head.append(
                dict(right=half(right), low=low_off, last=last, kdec=half(k * jnp.exp(last - cumc)))
            )
        hook()
        inv = unit_lower_inverses(diags)
        done = [[] for _ in range(heads)]
        own, cross = {}, {}
        for i in range(nblk):
            at = slice(i * BLOCK, (i + 1) * BLOCK)
            for h in range(heads):
                e, t = per_head[h], inv[h * nblk + i]
                own[h, i] = dot(t, e["right"][at])
                if i:
                    cross[h, i] = half(dot(t, e["low"][i - 1]))
        for i in range(nblk):
            for h in range(heads):
                u = own[h, i]
                if i:
                    u = u - dot(cross[h, i], jnp.concatenate(done[h], axis=0) if i > 1 else done[h][0])
                done[h].append(half(u))
        eye = iota((extent, extent), 0) == iota((extent, extent), 1)
        for h in range(heads):
            e = per_head[h]
            uw = jnp.concatenate(done[h], axis=0)
            r.ubuf[s, h] = uw
            fin = dot(uw, e["kdec"], TN)
            step = half(jnp.where(eye, jnp.exp(e["last"]) - 1.0, 0.0) - fin[extent:])
            state = half(fin[:extent])
            for f in range(2):
                r.out1[s, 2 * h + f, 0:extent, :] = step
                r.out1[s, 2 * h + f, extent:, :] = state[f * hv : (f + 1) * hv]
        for d in (2, 1, 3):
            x_copy(s, peer_x(d)).start()
        r.in1[s, x] = r.out1[s, x]
        after()

    def outputs_of(s):
        causal = iota((BLOCK, BLOCK), 0) >= iota((BLOCK, BLOCK), 1)
        for h in range(heads):
            lanes = slice(h * extent, (h + 1) * extent)
            q = unit_rows(r.rows[s, 0, :, lanes].astype(f32))
            kh = half(unit_rows(r.rows[s, 1, :, lanes].astype(f32)))
            cumc, cumr = r.cum_col[s, :, h : h + 1], r.cum_row[s, h : h + 1, :]
            qh, qg = half(q), q * jnp.exp(cumc)
            for i in range(nblk):
                at, before = slice(i * BLOCK, (i + 1) * BLOCK), slice(0, i * BLOCK)
                diff = cumc[at] - cumr[:, at]
                w_d = jnp.where(causal, jnp.exp(jnp.where(causal, diff, 0.0)), 0.0)
                out = dot(half(dot(qh[at], kh[at], NT) * w_d), r.ubuf[s, h, at])
                if i:
                    w_o = jnp.exp(cumc[at] - cumr[:, before])
                    out = out + dot(half(dot(qh[at], kh[before], NT) * w_o), r.ubuf[s, h, before])
                r.local_out[s, h, at, :] = out[:, :extent]
                r.reach[s, h, at, :] = half(qg[at] - out[:, extent:])
            gate = r.rows[s, 3, :, h * extent : (h + 1) * extent].astype(f32)
            r.gated[s, h] = gate * jax.nn.sigmoid(gate) * r.gain[...]


    def compose(prefix, step):
        e = step[0:extent]
        return prefix + dot(half(prefix), e) + step.astype(f32)

    def quad_copy(s, j, source, part):
        return pltpu.make_async_remote_copy(
            src_ref=r.in2.at[s, source, part], dst_ref=r.in2.at[s, source, part],
            send_sem=r.send2.at[s, j], recv_sem=r.recv2.at[s, source],
            device_id=sp_id(z - zl + j, x), device_id_type=MESH,
        )

    whole, state_only = pl.ds(0, box), pl.ds(extent, hv)

    def quad_each(s, act):
        for j in (3, 2, 1, 0):
            if j:

                @pl.when(is_b)
                def _():
                    act(quad_copy(s, j, zl, state_only))

                @pl.when(jnp.logical_and(zl < j, jnp.logical_not(is_b)))
                def _():
                    act(quad_copy(s, j, zl, whole))
            else:

                @pl.when(zl > 0)
                def _():
                    act(quad_copy(s, 0, zl, whole))

    def quad_arrive(s, j):
        if j == 0:

            @pl.when(jnp.logical_and(zl > 0, lower_quad))
            def _():
                quad_copy(s, 0, 0, state_only).wait_recv()

            @pl.when(jnp.logical_and(zl > 0, jnp.logical_not(lower_quad)))
            def _():
                quad_copy(s, 0, 0, whole).wait_recv()
        else:

            @pl.when(jnp.logical_or(zl > j, zl == 0))
            def _():
                quad_copy(s, 0, j, whole).wait_recv()

    def combine_group(s):
        for j in range(GROUP):

            @pl.when(x != j)
            def _():
                pltpu.make_async_remote_copy(
                    src_ref=r.out1.at[s, 0], dst_ref=r.in1.at[s, j], send_sem=r.send1.at[s, 0],
                    recv_sem=r.recv1.at[s, j], device_id=sp_id(z, j), device_id_type=MESH,
                ).wait_recv()

        prefix = r.in1[s, 0].astype(f32)
        for j in range(1, GROUP):
            r.gpre[s, j - 1] = prefix
            prefix = compose(prefix, r.in1[s, j])
        r.in2[s, zl] = half(prefix)
        quad_each(s, lambda copy: copy.start())

    def spread_copy(s, k):
        return pltpu.make_async_remote_copy(
            src_ref=r.s4_out.at[s], dst_ref=r.s4_in.at[s], send_sem=r.send3.at[s, k],
            recv_sem=r.recv3.at[s], device_id=sp_id(spread_to(k), x), device_id_type=MESH,
        )

    def state_copy(s, xx):
        return pltpu.make_async_remote_copy(
            src_ref=r.st_out.at[s, xx], dst_ref=r.st_in.at[s, x], send_sem=r.send4.at[s, xx],
            recv_sem=r.recv4.at[s, x], device_id=sp_id(z, xx), device_id_type=MESH,
        )

    def give_states(s, states):
        for xx in range(GROUP):
            r.st_out[s, xx] = half(states[xx])
        for d in (2, 1, 3):
            state_copy(s, peer_x(d)).start()
        r.st_in[s, x] = r.st_out[s, x]

    def with_groups(mine, mine_h, take, s):
        comps = [mine]
        for j in range(1, GROUP):
            g = r.gpre[s, j - 1]
            comps.append(mine + dot(mine_h, half(g[0:extent])) + g[take])
        return comps

    def combine_lower(s):
        r.qs[0] = jnp.zeros((hv, extent), f32)

        def give():
            mine = r.qs[zl]
            give_states(s, with_groups(mine, half(mine), slice(extent, box), s))

        @pl.when(is_b)
        def _():
            give()

        for j in range(GROUP):

            @pl.when(jnp.logical_or(zl > j, spreads))
            def _():
                quad_arrive(s, j)
                step = r.in2[s, j, extent:].astype(f32)
                if j:
                    state = r.qs[j]
                    step = state + dot(half(state), r.in2[s, j, 0:extent]) + step
                r.qs[j + 1] = step

        @pl.when(spreads)
        def _():
            r.s4_out[s] = half(r.qs[GROUP])
            for k in range(2):
                spread_copy(s, k).start()

        @pl.when(jnp.logical_not(is_b))
        def _():
            give()

    ends = jnp.logical_or(zl == 0, zl == GROUP - 1)

    def combine_upper(s):
        r.qpre[0] = jnp.zeros((box, extent), f32)
        for j in range(GROUP):

            @pl.when(jnp.logical_or(zl > j, ends))
            def _():
                quad_arrive(s, j)
                got = r.in2[s, j]
                r.qpre[j + 1] = got.astype(f32) if j == 0 else compose(r.qpre[j], got)

        @pl.when(ends)
        def _():
            r.qtot[s] = r.qpre[GROUP]

        mine = r.qpre[zl]
        comps = with_groups(mine, half(mine), slice(0, box), s)
        for j in range(GROUP):
            r.comp_d[s, j] = half(comps[j][0:extent])
            r.comp_c[s, j] = comps[j][extent:]

    def combine_quad(s):
        @pl.when(lower_quad)
        def _():
            combine_lower(s)

        @pl.when(jnp.logical_not(lower_quad))
        def _():
            combine_upper(s)

    tails = jnp.logical_or(z == GROUP, z == 2 * GROUP - 1)

    def tail_z(i):
        return jnp.where(z == GROUP, (3, 2, 5, 4)[i], (0, 1, 6, 7)[i])

    def tail_copy(s, i, xx):
        return pltpu.make_async_remote_copy(
            src_ref=r.tail_out.at[s, i * GROUP + xx], dst_ref=r.tail_in.at[s, x],
            send_sem=r.send_t.at[s, i * GROUP + xx], recv_sem=r.recv_t.at[s, x],
            device_id=sp_id(tail_z(i), xx), device_id_type=MESH,
        )

    def tail_each(s, act):
        for i in range(GROUP):
            for d in (2, 1, 3, 0):
                if i < GROUP - 1 or d:
                    act(tail_copy(s, i, peer_x(d)))

    def prepare_read(s):
        shape = r.nq.shape
        mine = (iota(shape, 0) == s) & (iota(shape, 1) == x // 2)

        def own(ref):
            kept = jnp.where(mine, ref[...].astype(f32), 0.0)
            return jnp.sum(jnp.sum(kept, axis=0), axis=0, keepdims=True)

        qn, kn = unit_rows(own(r.nq)), unit_rows(own(r.nk))
        r.pair_row[s, 0:1] = own(r.nv)
        r.pair_row[s, 1:2] = jnp.broadcast_to(jnp.sum(kn * qn, axis=-1, keepdims=True), (1, extent))
        for i, row in enumerate((qn, kn)):
            r.pair_col[s, i] = jnp.broadcast_to(row, (extent, extent)).T

    def tail(s, s4, s4h):
        tot = r.qtot[s]
        memory = half(s4 + dot(s4h, half(tot[0:extent])) + tot[extent:]).astype(f32)
        twice = jnp.concatenate([memory, memory], axis=0).T
        recall = jnp.sum(twice * r.pair_col[s, 0], axis=0, keepdims=True)
        retrieve = jnp.sum(twice * r.pair_col[s, 1], axis=0, keepdims=True)
        beta_new, decay_new = r.nb[s, x // 2], r.nd[s, x // 2]
        fresh = r.pair_row[s, 0:1] - decay_new * retrieve
        kept = (iota((1, extent), 1) // hv) == lax.rem(x, 2)
        read = jnp.where(kept, decay_new * recall + (beta_new * r.pair_row[s, 1:2]) * fresh, 0.0)
        r.memt[...] = jnp.where(kept, twice, 0.0)
        answer = jnp.broadcast_to(read, (4, extent))
        for i in range(GROUP):
            base = pl.multiple_of(tail_z(i) * 16, 16)
            keys = r.memt[pl.ds(base, 16), :]
            for xx in range(GROUP):
                r.tail_out[s, i * GROUP + xx, 0:4] = keys[xx * 4 : xx * 4 + 4]
                r.tail_out[s, i * GROUP + xx, 4:8] = answer
        tail_each(s, lambda copy: copy.start())
        r.tail_in[s, x] = r.tail_out[s, (GROUP - 1) * GROUP + x]

    def upper(s):
        @pl.when(jnp.logical_not(lower_quad))
        def _():
            pltpu.make_async_remote_copy(
                src_ref=r.s4_out.at[s], dst_ref=r.s4_in.at[s], send_sem=r.send3.at[s, 0],
                recv_sem=r.recv3.at[s], device_id=sp_id(spread_from, x), device_id_type=MESH,
            ).wait_recv()
            s4h = r.s4_in[s]
            s4 = s4h.astype(f32)

            @pl.when(tails)
            def _():
                tail(s, s4, s4h)

            give_states(s, [s4 + dot(s4h, r.comp_d[s, j]) + r.comp_c[s, j] for j in range(GROUP)])

    def finish(s):
        for o in range(GROUP):

            @pl.when(x != o)
            def _():
                pltpu.make_async_remote_copy(
                    src_ref=r.st_out.at[s, 0], dst_ref=r.st_in.at[s, o], send_sem=r.send4.at[s, 0],
                    recv_sem=r.recv4.at[s, o], device_id=sp_id(z, o), device_id_type=MESH,
                ).wait_recv()

        for h in range(heads):
            state_t = jnp.concatenate([r.st_in[s, 2 * h], r.st_in[s, 2 * h + 1]], axis=0)
            o = r.local_out[s, h] + dot(r.reach[s, h], state_t, NT)
            norm = lax.rsqrt(jnp.mean(o * o, axis=-1, keepdims=True) + norm_floor)
            r.mixed[s, :, h * extent : (h + 1) * extent] = half(o * norm * r.gated[s, h])

    def last_read(s):
        from_z = jnp.where((z >= 2) & (z < 6), GROUP, 2 * GROUP - 1)
        for o in range(GROUP):

            @pl.when(jnp.logical_not((z == from_z) & (x == o)))
            def _():
                pltpu.make_async_remote_copy(
                    src_ref=r.tail_out.at[s, 0], dst_ref=r.tail_in.at[s, o], send_sem=r.send_t.at[s, 0],
                    recv_sem=r.recv_t.at[s, o], device_id=sp_id(from_z, o), device_id_type=MESH,
                ).wait_recv()

        for h in range(heads):
            both = r.tail_in[s, 2 * h] + r.tail_in[s, 2 * h + 1]
            r.cache[s, h] = half(both[0:4])
            read = both[4:5]
            norm = lax.rsqrt(jnp.mean(read * read, axis=-1, keepdims=True) + norm_floor)
            r.first[s : s + 1, h * extent : (h + 1) * extent] = read * norm * r.gain[...]

    def phase(name, step, *args):
        with jax.named_scope(name):
            step(*args)

    def nothing():
        pass

    def group0_early():
        pl.semaphore_wait(r.relay_z.at[1], 2)
        phase("group0", combine_group, 0)

    phase("begin", begin)
    phase("near", near)
    phase("nf0", near_first, 0)
    phase("u0a", use, [0], [(2, 0), (4, 1)])
    phase("ns0", near_second, 0)
    phase("own1a", start_own, 1, 0)
    phase("cf0", cross_first, 0)
    phase("u0b", use, [0], [(3, 0), (5, 1), (2, 1), (4, 0)])
    phase("own1b", start_own, 1, 1)
    phase("far0", far, 0)
    phase("cs0", cross_second, 0)
    phase("u0c", use, [0], [(3, 1), (5, 0), (6, 0), (6, 1)])
    phase("nf1", near_first, 1)
    phase("cfar0", cross_far, 0)
    phase("u0d", use, [0], [(7, 0), (7, 1)])
    phase("rows0", round_rows, 0)
    phase("local0", local, 0, lambda: phase("ns1", near_second, 1), lambda: phase("far1", far, 1))
    phase("u1a", use, [1], [(2, 0), (4, 1), (2, 1), (4, 0)])
    phase("cc1", cross_first, 1)
    phase("cs1", cross_second, 1)
    phase("u1b", use, [1], [(3, 0), (5, 1), (3, 1), (5, 0)])
    phase("u1c", use, [1], [(6, 0), (6, 1)])
    phase("cfar1", cross_far, 1)
    phase("u1d", use, [1], [(7, 0), (7, 1)])
    phase("rows1", round_rows, 1)
    phase("local1", local, 1, nothing, group0_early)
    for s in range(seqs):
        phase(f"outs{s}", outputs_of, s)

    @pl.when(tails)
    def _():
        for s in range(seqs):
            prepare_read(s)

    phase("group1", combine_group, 1)
    phase("quad0", combine_quad, 0)
    phase("upper0", upper, 0)
    phase("quad1", combine_quad, 1)
    phase("finish0", finish, 0)
    phase("upper1", upper, 1)
    phase("finish1", finish, 1)
    phase("read0", last_read, 0)
    phase("read1", last_read, 1)

    for s in range(seqs):
        for i in range(2):
            own_partner(s, i).wait_send()
            forward(s, i).wait_send()
            for step in range(2):
                own_send(s, i, step).wait_send()
        for i in range(3):
            for hf in range(2):
                partner_send(s, i, hf).wait_send()
        for d in range(1, GROUP):
            x_copy(s, peer_x(d)).wait_send()
            state_copy(s, peer_x(d)).wait_send()
        quad_each(s, lambda copy: copy.wait_send())

        @pl.when(spreads)
        def _():
            for k in range(2):
                spread_copy(s, k).wait_send()

        @pl.when(tails)
        def _():
            tail_each(s, lambda copy: copy.wait_send())


def put_kernel(*refs):
    sems = refs[6]
    copies = [pltpu.make_async_copy(refs[i], refs[3 + i], sems.at[i]) for i in range(3)]
    for copy in copies:
        copy.start()
    for copy in copies:
        copy.wait()


def put(arrays):
    return pl.pallas_call(
        put_kernel,
        out_shape=tuple(jax.ShapeDtypeStruct(a.shape, a.dtype) for a in arrays),
        in_specs=[pl.BlockSpec(memory_space=pltpu.VMEM)] * 3,
        out_specs=(pl.BlockSpec(memory_space=pltpu.HBM),) * 3,
        scratch_shapes=[pltpu.SemaphoreType.DMA((3,))],
        compiler_params=pltpu.CompilerParams(vmem_limit_bytes=2 * 1024 * 1024),
        name="put",
    )(*arrays)


def shards(
    tokens, query_weight, key_weight, value_weight, gate_weight, beta_weight, decay_weight,
    beta_bias, rate_log, out_gain, new_query, new_key, new_value, new_beta, new_decay,
):
    seqs, span, kd = tokens.shape
    heads = rate_log.shape[0]
    extent = out_gain.shape[0]
    depth, width = query_weight.shape
    kc = kd // 2
    hv, box = extent // 2, extent + extent // 2
    key_rows = extent // lax.axis_size("sp")
    vmem = pl.BlockSpec(memory_space=pltpu.VMEM)
    hbm = pl.BlockSpec(memory_space=pltpu.HBM)
    inputs = ["x", "wq", "wk", "wv", "wg"] + [n + "_hbm" for n in SMALL]
    outputs = dict(
        mixed=jax.ShapeDtypeStruct((seqs, span, width), bf16),
        cache=jax.ShapeDtypeStruct((seqs, heads, key_rows, extent), bf16),
        first=jax.ShapeDtypeStruct((seqs, width), f32),
    )
    dma = pltpu.SemaphoreType.DMA
    scratch = dict(
        bw=pltpu.VMEM((heads, depth), bf16),
        dw=pltpu.VMEM((heads, depth), bf16),
        bias=pltpu.SMEM((heads,), f32),
        rate=pltpu.SMEM((heads,), f32),
        gain=pltpu.VMEM((1, extent), f32),
        nq=pltpu.VMEM((seqs, heads, extent), bf16),
        nk=pltpu.VMEM((seqs, heads, extent), bf16),
        nv=pltpu.VMEM((seqs, heads, extent), bf16),
        nb=pltpu.SMEM((seqs, heads), f32),
        nd=pltpu.SMEM((seqs, heads), f32),
        small_sem=dma((len(SMALL),)),
        bd=pltpu.VMEM((2 * PAD, depth), bf16),
        xs=pltpu.VMEM((8, 2, seqs * span, kc), bf16),
        wbuf=pltpu.VMEM((4, 8, kd, width), bf16),
        acc=pltpu.VMEM((4, seqs * span, width), f32),
        sacc=pltpu.VMEM((seqs, 2 * PAD, span), f32),
        rows=pltpu.VMEM((seqs, 4, span, width), bf16),
        cum_row=pltpu.VMEM((seqs, PAD, span), f32),
        cum_col=pltpu.VMEM((seqs, span, PAD), f32),
        ubuf=pltpu.VMEM((seqs, heads, span, 2 * extent), bf16),
        local_out=pltpu.VMEM((seqs, heads, span, extent), f32),
        reach=pltpu.VMEM((seqs, heads, span, extent), bf16),
        gated=pltpu.VMEM((seqs, heads, span, extent), f32),
        out1=pltpu.VMEM((seqs, GROUP, box, extent), bf16),
        in1=pltpu.VMEM((seqs, GROUP, box, extent), bf16),
        gpre=pltpu.VMEM((seqs, GROUP - 1, box, extent), f32),
        in2=pltpu.VMEM((seqs, GROUP, box, extent), bf16),
        qpre=pltpu.VMEM((GROUP + 1, box, extent), f32),
        qs=pltpu.VMEM((GROUP + 1, hv, extent), f32),
        pair_row=pltpu.VMEM((seqs, PAD, extent), f32),
        pair_col=pltpu.VMEM((seqs, 2, extent, extent), f32),
        relay_x=pltpu.SemaphoreType.REGULAR,
        relay_z=pltpu.SemaphoreType.REGULAR((2,)),
        qtot=pltpu.VMEM((seqs, box, extent), f32),
        comp_d=pltpu.VMEM((seqs, GROUP, extent, extent), bf16),
        comp_c=pltpu.VMEM((seqs, GROUP, hv, extent), f32),
        s4_out=pltpu.VMEM((seqs, hv, extent), bf16),
        s4_in=pltpu.VMEM((seqs, hv, extent), bf16),
        st_out=pltpu.VMEM((seqs, GROUP, hv, extent), bf16),
        st_in=pltpu.VMEM((seqs, GROUP, hv, extent), bf16),
        memt=pltpu.VMEM((extent, extent), f32),
        tail_out=pltpu.VMEM((seqs, GROUP * GROUP, PAD, extent), f32),
        tail_in=pltpu.VMEM((seqs, GROUP, PAD, extent), f32),
        tok_sem=dma((seqs, 2)),
        wsem=dma((4, 8)),
        own_sem=dma((2, seqs, 2)),
        fwd_sem=dma((2, seqs)),
        part_sem=dma((4, seqs, 2)),
        rx=dma((8, seqs, 2)),
        send1=dma((seqs, GROUP)),
        recv1=dma((seqs, GROUP)),
        send2=dma((seqs, GROUP)),
        recv2=dma((seqs, GROUP)),
        send3=dma((seqs, 2)),
        recv3=dma((seqs,)),
        send4=dma((seqs, GROUP)),
        recv4=dma((seqs, GROUP)),
        send_t=dma((seqs, GROUP * GROUP)),
        recv_t=dma((seqs, GROUP)),
    )
    names = inputs + list(outputs) + list(scratch)
    dims = (seqs, heads, span, extent, kc)

    def body(*refs):
        fused_kernel(names, dims, *refs)

    results = pl.pallas_call(
        body,
        out_shape=tuple(outputs.values()),
        in_specs=[hbm] * len(inputs),
        out_specs=(vmem,) * 3,
        scratch_shapes=list(scratch.values()),
        compiler_params=pltpu.CompilerParams(
            collective_id=0, has_side_effects=True, vmem_limit_bytes=32 * 1024 * 1024
        ),
        name="fused",
    )(
        *(
            pltpu.with_memory_space_constraint(value, pltpu.HBM)
            for value in (
                tokens, query_weight, key_weight, value_weight, gate_weight, beta_weight.T, decay_weight.T,
                beta_bias, rate_log, out_gain[None], new_query, new_key, new_value, new_beta, new_decay,
            )
        )
    )
    return put(results)


def solution(mesh):
    placed = (
        P(None, "sp", "tp"),
        P(None, "tp"),
        P(None, "tp"),
        P(None, "tp"),
        P(None, "tp"),
        P(None, "tp"),
        P(None, "tp"),
        P("tp"),
        P("tp"),
        P(),
        P(None, "tp", None),
        P(None, "tp", None),
        P(None, "tp", None),
        P(None, "tp"),
        P(None, "tp"),
    )
    return jax.shard_map(
        shards,
        mesh=mesh,
        in_specs=placed,
        out_specs=(P(None, "sp", "tp"), P(None, "tp", "sp", None), P(None, "tp")),
        check_vma=False,
    )
```
